32 devices in a mesh: sp: 4 (over z), fs: 4 (over y, x), tp: 2 (over core).
Axes of the slice: x: 2, y: 2, z: 4, core: 2. Of those that a mesh axis runs over, the one named last changes fastest.
Arguments:
- activations: bfloat16 [2048, 4096], P(('fs', 'sp'), 'tp'), parts along dimension 0, may hold values from -6 to 6
- input_norm_gain: float32 [4096], replicated, may hold values from 0.1 to 1.9
- window_query_weight: bfloat16 [4096, 2048], P('sp', 'tp'), may hold values from -0.09375 to 0.09375
- window_key_weight: bfloat16 [4096, 512], P('sp', 'tp'), may hold values from -0.09375 to 0.09375
- window_value_weight: bfloat16 [4096, 512], P('sp', 'tp'), may hold values from -0.09375 to 0.09375
- linear_query_weight: bfloat16 [4096, 1024], P('sp', 'tp'), may hold values from -0.09375 to 0.09375
- linear_key_weight: bfloat16 [4096, 1024], P('sp', 'tp'), may hold values from -0.09375 to 0.09375
- linear_value_weight: bfloat16 [4096, 2048], P('sp', 'tp'), may hold values from -0.09375 to 0.09375
- decay_down_factor: bfloat16 [4096, 16], replicated, may hold values from -0.09375 to 0.09375
- decay_up_factor: bfloat16 [16, 1024], P(None, 'tp'), may hold values from -1.5 to 1.5
- decay_offset_bias: float32 [1024], P('tp'), may hold values from -0.5 to 9
- extra_fading_exponent: float32 [2048, 8], P(('fs', 'sp'), 'tp'), parts along dimension 0, may hold values from -1.5 to 0
- starting_state: float32 [8, 128, 256], P('tp'), may hold values from -12 to 12
- head_sink_logit: float32 [32], P('tp'), may hold values from 1 to 5
- linear_head_gain: float32 [256], replicated, may hold values from 0.1 to 1.9
- window_output_weight: bfloat16 [2048, 4096], P('tp', 'sp'), may hold values from -0.09375 to 0.09375
- linear_output_weight: bfloat16 [2048, 4096], P('tp', 'sp'), may hold values from -0.09375 to 0.09375
Outputs:
- mixer_output: bfloat16 [2048, 4096], P(('fs', 'sp', 'tp')), parts along dimension 0
The draws below stay inside these ranges and needn't reach their ends.
There are 4 independent parts, one for each index of `fs`. The reference program is written for one: setup_inputs(seed, part) draws one part's arguments, and reference() takes and returns one part's arrays. A program takes and returns all parts, laid end to end along the dimension named above; an argument that names none is the same for every part. Nothing has to cross between parts.
All inputs are finite; a program needn't handle non-finite values.
Results may differ from the reference program's by a relative error of at most 0.019.
Values may be sent and summed in bfloat16 or wider, within the bound.
A program may use at most 128 MiB of HBM per device.

```python
import jax
import jax.numpy as jnp
from jax import lax

D = 4096
QH = 32
KVH = 8
HD = 64
WINDOW = 128
GATED_MIXERS = 8
LOOKUP_FEATURES = 128
DV = 256
RANK = 16
SPAN = 64
T_DEV = 128
TOKENS = 512
N_TP = 2


def draw_decay_offset_bias(key, part):
    key_flags, key_slow, key_quick = jax.random.split(key, 3)
    fast_share = 0.5
    is_quick = jax.random.uniform(key_flags, (GATED_MIXERS, 1)) < fast_share
    slow_values = jax.random.uniform(key_slow, (GATED_MIXERS, LOOKUP_FEATURES), minval=6.0, maxval=9.0)
    quick_values = jax.random.uniform(key_quick, (GATED_MIXERS, LOOKUP_FEATURES), minval=-0.5, maxval=1.0)
    return jnp.where(is_quick, quick_values, slow_values).reshape(GATED_MIXERS * LOOKUP_FEATURES).astype(jnp.float32)


def draw_extra_fading_exponent(key, part):
    key_rate, key_place, key_depth = jax.random.split(key, 3)
    block_count = TOKENS // T_DEV
    low_end = 0.25
    rates = jnp.exp(jax.random.uniform(key_rate, (block_count, GATED_MIXERS), minval=jnp.log(low_end), maxval=0.0))
    equilibrium_memory = jnp.repeat(-0.8 * rates / TOKENS, T_DEV, axis=0)
    element_indices = jax.random.randint(key_place, (2, GATED_MIXERS), 0, TOKENS)
    accrued_fading_totals = jnp.log(jax.random.uniform(key_depth, (2, GATED_MIXERS), minval=0.5, maxval=0.8))
    element_ordinals = jnp.arange(TOKENS, dtype=jnp.int32)[:, None, None]
    spike_contributions = jnp.sum(jnp.where(element_ordinals == element_indices[None], accrued_fading_totals[None], 0.0), axis=1)
    return (equilibrium_memory + spike_contributions).astype(jnp.float32)


def levels(rng, shape, shards, low, top_value):
    def one(axis_at, blocks):
        heights = jax.random.uniform(jax.random.fold_in(jax.random.fold_in(rng, 6), axis_at), (blocks,), jnp.float32, low / len(shards), top_value / len(shards))
        return jnp.repeat(jnp.exp(heights), shape[axis_at] // blocks).reshape((-1,) + (1,) * (len(shape) - axis_at - 1))

    factor_of = one(*shards[0])
    for cut in shards[1:]:
        factor_of = factor_of * one(*cut)
    return factor_of


def scatter_about(stream_key, dims, spread, bound, shards=(), kind=jnp.bfloat16):
    level = levels(stream_key, dims, shards, -0.22, 0.18) if shards else 1.0
    values = jax.random.normal(stream_key, dims, jnp.float32) * spread * level
    return jnp.minimum(jnp.maximum(values, -bound), bound).astype(kind)


def setup_inputs(seed: int = 0, part: int = 0) -> dict:
    seeds = jax.random.split(jax.random.key(seed), 18)
    part_splits = jax.random.split(jax.random.fold_in(seeds[17], part), 18)
    activations = scatter_about(part_splits[0], (TOKENS, D), 1.0, 6.0, ((0, 4), (1, 2)))
    input_norm_gain = jnp.clip(1.0 + 0.18 * jax.random.normal(seeds[1], (D,), jnp.float32), 0.1, 1.9)
    window_query_weight = scatter_about(seeds[2], (D, QH * HD), D ** -0.5, 0.09375, ((0, 4), (1, 2)))
    window_key_weight = scatter_about(seeds[3], (D, KVH * HD), D ** -0.5, 0.09375, ((0, 4), (1, 2)))
    window_value_weight = scatter_about(seeds[4], (D, KVH * HD), D ** -0.5, 0.09375, ((0, 4), (1, 2)))
    linear_query_weight = scatter_about(seeds[5], (D, GATED_MIXERS * LOOKUP_FEATURES), D ** -0.5, 0.09375, ((0, 4), (1, 2)))
    linear_key_weight = scatter_about(seeds[6], (D, GATED_MIXERS * LOOKUP_FEATURES), D ** -0.5, 0.09375, ((0, 4), (1, 2)))
    linear_value_weight = scatter_about(seeds[7], (D, GATED_MIXERS * DV), D ** -0.5, 0.09375, ((0, 4), (1, 2)))
    decay_down_factor = scatter_about(seeds[8], (D, RANK), D ** -0.5, 0.09375)
    decay_up_factor = scatter_about(seeds[9], (RANK, GATED_MIXERS * LOOKUP_FEATURES), RANK ** -0.5, 1.5, ((1, 2),))
    decay_offset_bias = draw_decay_offset_bias(jax.random.fold_in(seeds[17], 71), part)
    extra_fading_exponent = draw_extra_fading_exponent(jax.random.fold_in(jax.random.fold_in(seeds[17], part), 71), part)
    starting_state = scatter_about(seeds[12], (GATED_MIXERS, LOOKUP_FEATURES, DV), 2.0, 12.0, ((0, 2),), jnp.float32)
    head_sink_logit = jnp.clip(1.0 + 4.0 * jax.random.uniform(seeds[13], (QH,), jnp.float32) ** levels(seeds[13], (QH,), ((0, 2),), -0.2, 0.2), 1.0, 5.0)
    linear_head_gain = jnp.clip(1.0 + 0.18 * jax.random.normal(seeds[14], (DV,), jnp.float32), 0.1, 1.9)
    window_output_weight = scatter_about(seeds[15], (QH * HD, D), (QH * HD + GATED_MIXERS * DV) ** -0.5, 0.09375, ((0, 2), (1, 4)))
    linear_output_weight = scatter_about(seeds[16], (GATED_MIXERS * DV, D), (QH * HD + GATED_MIXERS * DV) ** -0.5, 0.09375, ((0, 2), (1, 4)))
    return {"activations": activations, "input_norm_gain": input_norm_gain, "window_query_weight": window_query_weight, "window_key_weight": window_key_weight, "window_value_weight": window_value_weight, "linear_query_weight": linear_query_weight, "linear_key_weight": linear_key_weight, "linear_value_weight": linear_value_weight, "decay_down_factor": decay_down_factor, "decay_up_factor": decay_up_factor, "decay_offset_bias": decay_offset_bias, "extra_fading_exponent": extra_fading_exponent, "starting_state": starting_state, "head_sink_logit": head_sink_logit, "linear_head_gain": linear_head_gain, "window_output_weight": window_output_weight, "linear_output_weight": linear_output_weight}


EPS = 1e-05
FADING_SOFTNESS = 16.0
HIGH_PRECISION = lax.Precision.HIGHEST

def window_reference(near_query, near_keys, near_values, head_sink_logit):
    stream_extent = near_query.shape[0]
    blocks = stream_extent // WINDOW
    groups = QH // KVH
    zeros_front = jnp.zeros((WINDOW, KVH * HD), jnp.float32)

    def banded(current):
        extended = jnp.concatenate([zeros_front, current.astype(jnp.float32)], axis=0)
        earlier = extended[:stream_extent].reshape(blocks, WINDOW, KVH, HD)
        present = extended[WINDOW:].reshape(blocks, WINDOW, KVH, HD)
        return jnp.concatenate([earlier, present], axis=1)
    key_band = banded(near_keys)
    value_band = banded(near_values)
    queries = near_query.astype(jnp.float32).reshape(blocks, WINDOW, KVH, groups, HD)
    scores = jnp.einsum('nqhgd,nkhd->hgnqk', queries, key_band, precision=HIGH_PRECISION) * HD ** (-0.5)
    head_ids = jnp.arange(QH, dtype=jnp.int32)
    slopes = jnp.exp2(-8.0 * (head_ids + 1).astype(jnp.float32) / QH).reshape(KVH, groups)
    query_pos = jnp.arange(WINDOW, dtype=jnp.int32)
    key_pos = jnp.arange(2 * WINDOW, dtype=jnp.int32)
    distance = query_pos[:, None] - key_pos[None, :] + WINDOW
    start_pos = (jnp.arange(blocks, dtype=jnp.int32) - 1) * WINDOW
    absolute = start_pos[:, None] + key_pos[None, :]
    allowed = ((distance >= 0) & (distance < WINDOW))[None] & (absolute >= 0)[:, None, :]
    biased = scores - slopes[:, :, None, None, None] * distance.astype(jnp.float32)
    weights = jnp.where(allowed, jnp.exp(biased), 0.0)
    denominator = lax.optimization_barrier(jnp.sum(weights, axis=-1, keepdims=True)) + jnp.exp(head_sink_logit.reshape(KVH, groups))[:, :, None, None, None]
    attention = (weights / denominator).astype(jnp.bfloat16)
    attended = jnp.einsum('hgnqk,nkhd->nqhgd', attention.astype(jnp.float32), value_band, precision=HIGH_PRECISION)
    return attended.reshape(stream_extent, QH * HD).astype(jnp.bfloat16)

def linear_reference(gated_query, gated_keys, gated_values, fading_exponent, linear_head_gain, starting_state):
    stream_extent = gated_query.shape[0]
    span_count = stream_extent // SPAN
    scaled_query = gated_query.astype(jnp.float32).reshape(span_count, SPAN, GATED_MIXERS, LOOKUP_FEATURES) * LOOKUP_FEATURES ** (-0.5)
    keys_wide = gated_keys.astype(jnp.float32).reshape(span_count, SPAN, GATED_MIXERS, LOOKUP_FEATURES)
    values_wide = gated_values.astype(jnp.float32).reshape(span_count, SPAN, GATED_MIXERS, DV)
    running = jnp.cumsum(fading_exponent.reshape(span_count, SPAN, GATED_MIXERS, LOOKUP_FEATURES), axis=1)
    span_end = running[:, -1]
    query_with_decay = scaled_query * jnp.exp(running)
    inverse_keys = keys_wide * jnp.exp(-running)
    ending_keys = keys_wide * jnp.exp(span_end[:, None] - running)
    inner = jnp.einsum('nchk,nshk->nhcs', query_with_decay, inverse_keys, precision=HIGH_PRECISION)
    lower = jnp.tril(jnp.ones((SPAN, SPAN), dtype=bool))
    inner = jnp.where(lower, inner, 0.0)
    within = jnp.einsum('nhcs,nshv->nchv', inner, values_wide, precision=HIGH_PRECISION)

    def advance(running_state, inputs):
        query_portion, key_portion, value_portion, scale_factor = inputs
        layer_output = jnp.einsum('fmy,mys->fms', query_portion, running_state, precision=HIGH_PRECISION)
        running_state = running_state * scale_factor[..., None] + jnp.einsum('gxp,gxz->xpz', key_portion, value_portion, precision=HIGH_PRECISION)
        return (running_state, layer_output)
    start_state = starting_state.astype(jnp.float32)
    final_state, carried = lax.scan(advance, start_state, (query_with_decay, ending_keys, values_wide, jnp.exp(span_end)))
    flat = (within + carried).reshape(stream_extent, GATED_MIXERS, DV)
    normal = flat * lax.rsqrt(lax.optimization_barrier(jnp.mean(flat * flat, axis=-1, keepdims=True)) + EPS) * linear_head_gain
    return normal.reshape(stream_extent, GATED_MIXERS * DV).astype(jnp.bfloat16)

def reference(activations, input_norm_gain, window_query_weight, window_key_weight, window_value_weight, linear_query_weight, linear_key_weight, linear_value_weight, decay_down_factor, decay_up_factor, decay_offset_bias, extra_fading_exponent, starting_state, head_sink_logit, linear_head_gain, window_output_weight, linear_output_weight):
    widened = activations.astype(jnp.float32)
    normed = (widened * lax.rsqrt(lax.optimization_barrier(jnp.mean(widened * widened, axis=1, keepdims=True)) + EPS) * input_norm_gain).astype(jnp.bfloat16)

    def project(matrix):
        return jnp.dot(normed, matrix, preferred_element_type=jnp.float32).astype(jnp.bfloat16)
    near_query = project(window_query_weight)
    near_keys = project(window_key_weight)
    near_values = project(window_value_weight)
    gated_query = project(linear_query_weight)
    gated_keys = project(linear_key_weight)
    gated_values = project(linear_value_weight)
    low_rank = project(decay_down_factor)
    attention_energies = jnp.dot(low_rank, decay_up_factor, preferred_element_type=jnp.float32) + decay_offset_bias
    stream_extent = normed.shape[0]
    fading_exponent = (jax.nn.log_sigmoid(attention_energies) / FADING_SOFTNESS).reshape(stream_extent, GATED_MIXERS, LOOKUP_FEATURES) + extra_fading_exponent[:, :, None]
    near_out = window_reference(near_query, near_keys, near_values, head_sink_logit)
    gated_out = linear_reference(gated_query, gated_keys, gated_values, fading_exponent, linear_head_gain, starting_state)
    window_cols = QH * HD // N_TP
    linear_cols = GATED_MIXERS * DV // N_TP
    accumulated = jnp.zeros((stream_extent, D), jnp.float32)
    for member in range(N_TP):
        first_w = member * window_cols
        first_l = member * linear_cols
        partial_value = jnp.dot(near_out[:, first_w:first_w + window_cols], window_output_weight[first_w:first_w + window_cols], preferred_element_type=jnp.float32)
        partial_value = partial_value + jnp.dot(gated_out[:, first_l:first_l + linear_cols], linear_output_weight[first_l:first_l + linear_cols], preferred_element_type=jnp.float32)
        rounded = lax.optimization_barrier(partial_value.astype(jnp.bfloat16))
        accumulated = accumulated + rounded.astype(jnp.float32)
    return accumulated.astype(jnp.bfloat16)
```

```python
import jax
import jax.numpy as jnp
from jax import lax
from jax.sharding import PartitionSpec as P

QH = 32
HD = 64
WINDOW = 128
LOOKUP_FEATURES = 128
DV = 256
SPAN = 64
KVH = 8
GATED_MIXERS = 8


EPS = 1e-05
FADING_SOFTNESS = 16.0
HIGH_PRECISION = lax.Precision.HIGHEST


def passed_along(value, axis, steps):
    count = lax.axis_size(axis)
    leading, last = (max(0, -steps), min(count, count - steps))
    return lax.ppermute(value, axis, [(source, source + steps) for source in range(leading, last)])


def prefix(x, axis, combine, identity):
    peers, place = (lax.axis_size(axis), lax.axis_index(axis))
    everything = jax.tree.map(
        lambda part, kind: lax.all_gather(part.astype(kind), axis), x, (jnp.bfloat16, jnp.bfloat16)
    )
    start = jax.tree.map(
        lambda part, zero: jnp.broadcast_to(jnp.asarray(zero, part.dtype), part.shape), x, identity
    )

    def hop(k, before):
        reached = k < place
        new = combine(
            before, jax.tree.map(lambda part, own: part[k].astype(own.dtype), everything, x)
        )
        return jax.tree.map(lambda a, b: jnp.where(reached, a, b), new, before)

    return lax.fori_loop(0, peers, hop, start)


def window_attention(near_query, near_keys, near_values, head_sink_logit):
    stream_extent = near_query.shape[0]
    key_heads = near_keys.shape[1] // HD
    heads_here = near_query.shape[1] // HD
    groups = heads_here // key_heads
    blocks = stream_extent // WINDOW
    tail_rows = jnp.stack([near_keys, near_values])
    before = passed_along(tail_rows, "sp", 1)

    def banded(previous, current):
        extended = jnp.concatenate([previous, current], axis=0)
        earlier = extended[:stream_extent].reshape(blocks, WINDOW, key_heads, HD)
        present = extended[WINDOW:].reshape(blocks, WINDOW, key_heads, HD)
        return jnp.concatenate([earlier, present], axis=1)

    key_band = banded(before[0], near_keys)
    value_band = banded(before[1], near_values)
    queries = near_query.reshape(blocks, WINDOW, key_heads, groups, HD)
    scores = jnp.einsum(
        "nqhgd,nkhd->hgnqk", queries, key_band, preferred_element_type=jnp.float32
    ) * HD ** (-0.5)
    head_ids = lax.axis_index("tp") * heads_here + jnp.arange(heads_here, dtype=jnp.int32)
    slopes = jnp.exp2(-8.0 * (head_ids + 1).astype(jnp.float32) / QH).reshape(key_heads, groups)
    query_pos = jnp.arange(WINDOW, dtype=jnp.int32)
    key_pos = jnp.arange(2 * WINDOW, dtype=jnp.int32)
    distance = query_pos[:, None] - key_pos[None, :] + WINDOW
    start_pos = (
        lax.axis_index("sp") * stream_extent + (jnp.arange(blocks, dtype=jnp.int32) - 1) * WINDOW
    )
    absolute = start_pos[:, None] + key_pos[None, :]
    allowed = ((distance >= 0) & (distance < WINDOW))[None] & (absolute >= 0)[:, None, :]
    biased = scores - slopes[:, :, None, None, None] * distance.astype(jnp.float32)
    weights = jnp.where(allowed, jnp.exp(biased), 0.0)
    denominator = (
        jnp.sum(weights, axis=-1, keepdims=True)
        + jnp.exp(head_sink_logit.reshape(key_heads, groups))[:, :, None, None, None]
    )
    attention = (weights / denominator).astype(jnp.bfloat16)
    attended = jnp.einsum(
        "hgnqk,nkhd->nqhgd", attention, value_band, preferred_element_type=jnp.float32
    )
    return attended.reshape(stream_extent, heads_here * HD).astype(jnp.bfloat16)


def linear_attention(
    gated_query, gated_keys, gated_values, fading_exponent, linear_head_gain, starting_state
):
    stream_extent = gated_query.shape[0]
    head_total = gated_query.shape[1] // LOOKUP_FEATURES
    span_count = stream_extent // SPAN
    scaled_query = gated_query.astype(jnp.float32).reshape(
        span_count, SPAN, head_total, LOOKUP_FEATURES
    ) * LOOKUP_FEATURES ** (-0.5)
    keys_wide = gated_keys.astype(jnp.float32).reshape(
        span_count, SPAN, head_total, LOOKUP_FEATURES
    )
    values_wide = gated_values.astype(jnp.float32).reshape(span_count, SPAN, head_total, DV)
    running = jnp.cumsum(
        fading_exponent.reshape(span_count, SPAN, head_total, LOOKUP_FEATURES), axis=1
    )
    span_end = running[:, -1]
    query_with_decay = scaled_query * jnp.exp(running)
    inverse_keys = keys_wide * jnp.exp(-running)
    ending_keys = keys_wide * jnp.exp(span_end[:, None] - running)
    inner = jnp.einsum("nchk,nshk->nhcs", query_with_decay, inverse_keys, precision=HIGH_PRECISION)
    lower = jnp.tril(jnp.ones((SPAN, SPAN), dtype=bool))
    inner = jnp.where(lower, inner, 0.0)
    within = jnp.einsum("nhcs,nshv->nchv", inner, values_wide, precision=HIGH_PRECISION)

    def advance(running_state, inputs):
        query_portion, key_portion, value_portion, scale_factor = inputs
        layer_output = jnp.einsum(
            "fmy,mys->fms", query_portion, running_state, precision=HIGH_PRECISION
        )
        running_state = running_state * scale_factor[..., None] + jnp.einsum(
            "gxp,gxz->xpz", key_portion, value_portion, precision=HIGH_PRECISION
        )
        return (running_state, layer_output)

    start_state = jnp.zeros((head_total, LOOKUP_FEATURES, DV), jnp.float32)
    state_end, carried = lax.scan(
        advance, start_state, (query_with_decay, ending_keys, values_wide, jnp.exp(span_end))
    )
    device_decay = jnp.exp(jnp.sum(span_end, axis=0))
    prefix_sums = jnp.cumsum(span_end, axis=0) - span_end

    def combine(earlier, later):
        return (earlier[0] * later[0], later[0][..., None] * earlier[1] + later[1])

    decay_before, state_before = prefix(
        (device_decay, state_end),
        "sp",
        combine,
        (jnp.ones_like(device_decay), jnp.zeros_like(state_end)),
    )
    incoming_rows = state_before + decay_before[..., None] * starting_state
    crossing = jnp.einsum(
        "qwso,soz->qwsz",
        query_with_decay * jnp.exp(prefix_sums)[:, None],
        incoming_rows,
        precision=HIGH_PRECISION,
    )
    flat = (within + carried + crossing).reshape(stream_extent, head_total, DV)
    normal = (
        flat * lax.rsqrt(jnp.mean(flat * flat, axis=-1, keepdims=True) + EPS) * linear_head_gain
    )
    return normal.reshape(stream_extent, head_total * DV).astype(jnp.bfloat16)


def local(
    activations,
    input_norm_gain,
    window_query_weight,
    window_key_weight,
    window_value_weight,
    linear_query_weight,
    linear_key_weight,
    linear_value_weight,
    decay_down_factor,
    decay_up_factor,
    decay_offset_bias,
    extra_fading_exponent,
    starting_state,
    head_sink_logit,
    linear_head_gain,
    window_output_weight,
    linear_output_weight,
):
    gathered = lax.all_gather(activations, "tp", axis=1, tiled=True)
    widened = gathered.astype(jnp.float32)
    normed = (
        widened
        * lax.rsqrt(jnp.mean(widened * widened, axis=1, keepdims=True) + EPS)
        * input_norm_gain
    ).astype(jnp.bfloat16)
    row_total = normed.shape[0]
    matrices = (
        window_query_weight,
        window_key_weight,
        window_value_weight,
        linear_query_weight,
        linear_key_weight,
        linear_value_weight,
    )
    segments = (
        lax.all_gather(matrices[0], "sp", axis=0, tiled=True),
        lax.all_gather(matrices[1], "sp", axis=0, tiled=True),
        lax.all_gather(matrices[2], "sp", axis=0, tiled=True),
        lax.all_gather(matrices[3], "sp", axis=0, tiled=True),
        lax.all_gather(matrices[4], "sp", axis=0, tiled=True),
        lax.all_gather(matrices[5], "sp", axis=0, tiled=True),
    )
    projected = tuple(
        (jnp.dot(normed, segment, preferred_element_type=jnp.float32) for segment in segments)
    )
    near_query, near_keys, near_values, gated_query, gated_keys, gated_values = [
        product.astype(jnp.bfloat16) for product in projected
    ]
    low_rank = jnp.dot(normed, decay_down_factor, preferred_element_type=jnp.float32).astype(
        jnp.bfloat16
    )
    attention_energies = (
        jnp.dot(low_rank, decay_up_factor, preferred_element_type=jnp.float32) + decay_offset_bias
    )
    head_total = extra_fading_exponent.shape[1]
    fading_exponent = (jax.nn.log_sigmoid(attention_energies) / FADING_SOFTNESS).reshape(
        row_total, head_total, LOOKUP_FEATURES
    ) + extra_fading_exponent[:, :, None]
    near_out = window_attention(near_query, near_keys, near_values, head_sink_logit)
    gated_out = linear_attention(
        gated_query, gated_keys, gated_values, fading_exponent, linear_head_gain, starting_state
    )
    window_full, linear_full = (
        lax.all_gather(window_output_weight, "sp", axis=1, tiled=True),
        lax.all_gather(linear_output_weight, "sp", axis=1, tiled=True),
    )
    return lax.psum_scatter(
        (
            jnp.dot(near_out, window_full, preferred_element_type=jnp.float32)
            + jnp.dot(gated_out, linear_full, preferred_element_type=jnp.float32)
        ).astype(jnp.bfloat16),
        "tp",
        scatter_dimension=0,
        tiled=True,
    )


def head_window(near_query, near_keys, near_values, head_sink_logit, first_head):
    stream_extent = near_query.shape[0]
    key_heads = near_keys.shape[1] // HD
    heads_here = near_query.shape[1] // HD
    groups = heads_here // key_heads
    blocks = stream_extent // WINDOW

    def banded(current):
        extended = jnp.concatenate(
            [jnp.zeros((WINDOW, current.shape[1]), current.dtype), current], axis=0
        )
        earlier = extended[:stream_extent].reshape(blocks, WINDOW, key_heads, HD)
        present = extended[WINDOW:].reshape(blocks, WINDOW, key_heads, HD)
        return jnp.concatenate([earlier, present], axis=1)

    key_band = banded(near_keys)
    value_band = banded(near_values)
    queries = near_query.reshape(blocks, WINDOW, key_heads, groups, HD)
    scores = jnp.einsum(
        "nqhgd,nkhd->hgnqk", queries, key_band, preferred_element_type=jnp.float32
    ) * HD ** (-0.5)
    head_ids = first_head + jnp.arange(heads_here, dtype=jnp.int32)
    slopes = jnp.exp2(-8.0 * (head_ids + 1).astype(jnp.float32) / QH).reshape(key_heads, groups)
    query_pos = jnp.arange(WINDOW, dtype=jnp.int32)
    key_pos = jnp.arange(2 * WINDOW, dtype=jnp.int32)
    distance = query_pos[:, None] - key_pos[None, :] + WINDOW
    absolute = (jnp.arange(blocks, dtype=jnp.int32) - 1)[:, None] * WINDOW + key_pos[None, :]
    allowed = ((distance >= 0) & (distance < WINDOW))[None] & (absolute >= 0)[:, None, :]
    biased = scores - slopes[:, :, None, None, None] * distance.astype(jnp.float32)
    weights = jnp.where(allowed, jnp.exp(biased), 0.0)
    denominator = (
        jnp.sum(weights, axis=-1, keepdims=True)
        + jnp.exp(head_sink_logit.reshape(key_heads, groups))[:, :, None, None, None]
    )
    attention = (weights / denominator).astype(jnp.bfloat16)
    attended = jnp.einsum(
        "hgnqk,nkhd->nqhgd", attention, value_band, preferred_element_type=jnp.float32
    )
    return attended.reshape(stream_extent, heads_here * HD).astype(jnp.bfloat16)


def head_linear(gated_query, gated_keys, gated_values, fading, gain, state):
    stream_extent = gated_query.shape[0]
    heads = gated_query.shape[1] // LOOKUP_FEATURES
    spans = stream_extent // SPAN
    bf = jnp.bfloat16

    def mm(spec, a, b):
        return jnp.einsum(spec, a.astype(bf), b.astype(bf), preferred_element_type=jnp.float32)

    queries = gated_query.astype(jnp.float32).reshape(
        spans, SPAN, heads, LOOKUP_FEATURES
    ) * LOOKUP_FEATURES ** (-0.5)
    keys = gated_keys.astype(jnp.float32).reshape(spans, SPAN, heads, LOOKUP_FEATURES)
    values = gated_values.reshape(spans, SPAN, heads, DV)
    running = jnp.cumsum(fading.reshape(spans, SPAN, heads, LOOKUP_FEATURES), axis=1)
    span_end = running[:, -1]
    decayed = queries * jnp.exp(running)
    inner = mm("nchk,nshk->nhcs", decayed, keys * jnp.exp(-running))
    inner = jnp.where(jnp.tril(jnp.ones((SPAN, SPAN), dtype=bool)), inner, 0.0)
    within = mm("nhcs,nshv->nchv", inner, values)
    added = mm("nshk,nshv->nhkv", keys * jnp.exp(span_end[:, None] - running), values)
    scale = jnp.exp(span_end)
    before = []
    for n in range(spans):
        before.append(state)
        state = state * scale[n][..., None] + added[n]
    carried = mm("nchk,nhkv->nchv", decayed, jnp.stack(before))
    flat = within + carried
    normal = flat * lax.rsqrt(jnp.mean(flat * flat, axis=-1, keepdims=True) + EPS) * gain
    return normal.reshape(stream_extent, heads * DV).astype(bf)


def stationary(
    activations,
    input_norm_gain,
    window_query_weight,
    window_key_weight,
    window_value_weight,
    linear_query_weight,
    linear_key_weight,
    linear_value_weight,
    decay_down_factor,
    decay_up_factor,
    decay_offset_bias,
    extra_fading_exponent,
    starting_state,
    head_sink_logit,
    linear_head_gain,
    window_output_weight,
    linear_output_weight,
):
    bf = jnp.bfloat16
    sp, tp = lax.axis_size("sp"), lax.axis_size("tp")
    me_sp, me_tp = lax.axis_index("sp"), lax.axis_index("tp")
    rows = activations.shape[0]
    tokens = rows * sp
    gathered = lax.all_gather(activations, "tp", axis=1, tiled=True)
    widened = gathered.astype(jnp.float32)
    normed = (
        widened
        * lax.rsqrt(jnp.mean(widened * widened, axis=1, keepdims=True) + EPS)
        * input_norm_gain
    ).astype(bf)
    low_own = jnp.dot(normed, decay_down_factor, preferred_element_type=jnp.float32).astype(bf)
    low_rank = lax.all_gather(low_own, "sp", axis=0, tiled=True)
    fade_own = lax.all_to_all(extra_fading_exponent, "sp", 1, 0, tiled=True)
    slices = lax.all_to_all(normed, "sp", 1, 0, tiled=True)
    matrices = (
        window_query_weight,
        window_key_weight,
        window_value_weight,
        linear_query_weight,
        linear_key_weight,
        linear_value_weight,
    )
    parts = [
        jnp.dot(slices, m, preferred_element_type=jnp.float32)
        .astype(bf)
        .reshape(tokens, sp, m.shape[1] // sp)
        .transpose(1, 0, 2)
        for m in matrices
    ]
    widths = [m.shape[1] // sp for m in matrices]
    joined = lax.psum_scatter(jnp.concatenate(parts, axis=2), "sp", scatter_dimension=0)
    pieces, at = [], 0
    for width in widths:
        pieces.append(joined[:, at : at + width])
        at += width
    near_query, near_keys, near_values, gated_query, gated_keys, gated_values = pieces
    heads = fade_own.shape[1]
    channels = heads * LOOKUP_FEATURES
    up = lax.dynamic_slice_in_dim(decay_up_factor, me_sp * channels, channels, 1)
    bias = lax.dynamic_slice_in_dim(decay_offset_bias, me_sp * channels, channels, 0)
    energies = jnp.dot(low_rank, up, preferred_element_type=jnp.float32) + bias
    fading = (jax.nn.log_sigmoid(energies) / FADING_SOFTNESS).reshape(
        tokens, heads, LOOKUP_FEATURES
    ) + fade_own[:, :, None]
    near_heads = near_query.shape[1] // HD
    sinks = lax.dynamic_slice_in_dim(head_sink_logit, me_sp * near_heads, near_heads, 0)
    near_out = head_window(
        near_query, near_keys, near_values, sinks, (me_tp * sp + me_sp) * near_heads
    )
    state = lax.dynamic_slice_in_dim(starting_state, me_sp * heads, heads, 0)
    gated_out = head_linear(
        gated_query, gated_keys, gated_values, fading, linear_head_gain, state
    )
    both = lax.all_gather(jnp.concatenate([near_out, gated_out], axis=1), "sp", axis=0)
    split = near_out.shape[1]
    near_full = both[:, :, :split].transpose(1, 0, 2).reshape(tokens, -1)
    gated_full = both[:, :, split:].transpose(1, 0, 2).reshape(tokens, -1)
    term = (
        jnp.dot(near_full, window_output_weight, preferred_element_type=jnp.float32)
        + jnp.dot(gated_full, linear_output_weight, preferred_element_type=jnp.float32)
    ).astype(bf)
    term = term.reshape(sp, tp, rows // tp, -1)
    summed = lax.psum_scatter(term, "tp", scatter_dimension=1)
    return lax.all_to_all(summed, "sp", 0, 2, tiled=True).reshape(rows // tp, -1)


def divides(sp, tp):
    return GATED_MIXERS % (sp * tp) == 0 and KVH % (sp * tp) == 0 and QH % (sp * tp) == 0


def solution(mesh):
    placed = (
        P(("fs", "sp"), "tp"),
        P(),
        P("sp", "tp"),
        P("sp", "tp"),
        P("sp", "tp"),
        P("sp", "tp"),
        P("sp", "tp"),
        P("sp", "tp"),
        P(),
        P(None, "tp"),
        P("tp"),
        P(("fs", "sp"), "tp"),
        P("tp", None, None),
        P("tp"),
        P(),
        P("tp", "sp"),
        P("tp", "sp"),
    )
    body = stationary if divides(mesh.shape["sp"], mesh.shape["tp"]) else local
    return jax.shard_map(
        body, mesh=mesh, in_specs=placed, out_specs=P(("fs", "sp", "tp"), None), check_vma=False
    )
```

```python
import functools

import jax
import jax.numpy as jnp
from jax import lax
from jax.experimental import pallas as pl
from jax.experimental.pallas import tpu as pltpu
from jax.sharding import PartitionSpec as P

QH = 32
HD = 64
WINDOW = 128
LOOKUP_FEATURES = 128
DV = 256
SPAN = 64
KVH = 8
GATED_MIXERS = 8


EPS = 1e-05
FADING_SOFTNESS = 16.0
HIGH_PRECISION = lax.Precision.HIGHEST


def passed_along(value, axis, steps):
    count = lax.axis_size(axis)
    leading, last = (max(0, -steps), min(count, count - steps))
    return lax.ppermute(value, axis, [(source, source + steps) for source in range(leading, last)])


def prefix(x, axis, combine, identity):
    peers, place = (lax.axis_size(axis), lax.axis_index(axis))
    everything = jax.tree.map(
        lambda part, kind: lax.all_gather(part.astype(kind), axis), x, (jnp.bfloat16, jnp.bfloat16)
    )
    start = jax.tree.map(
        lambda part, zero: jnp.broadcast_to(jnp.asarray(zero, part.dtype), part.shape), x, identity
    )

    def hop(k, before):
        reached = k < place
        new = combine(
            before, jax.tree.map(lambda part, own: part[k].astype(own.dtype), everything, x)
        )
        return jax.tree.map(lambda a, b: jnp.where(reached, a, b), new, before)

    return lax.fori_loop(0, peers, hop, start)


def window_attention(near_query, near_keys, near_values, head_sink_logit):
    stream_extent = near_query.shape[0]
    key_heads = near_keys.shape[1] // HD
    heads_here = near_query.shape[1] // HD
    groups = heads_here // key_heads
    blocks = stream_extent // WINDOW
    tail_rows = jnp.stack([near_keys, near_values])
    before = passed_along(tail_rows, "sp", 1)

    def banded(previous, current):
        extended = jnp.concatenate([previous, current], axis=0)
        earlier = extended[:stream_extent].reshape(blocks, WINDOW, key_heads, HD)
        present = extended[WINDOW:].reshape(blocks, WINDOW, key_heads, HD)
        return jnp.concatenate([earlier, present], axis=1)

    key_band = banded(before[0], near_keys)
    value_band = banded(before[1], near_values)
    queries = near_query.reshape(blocks, WINDOW, key_heads, groups, HD)
    scores = jnp.einsum(
        "nqhgd,nkhd->hgnqk", queries, key_band, preferred_element_type=jnp.float32
    ) * HD ** (-0.5)
    head_ids = lax.axis_index("tp") * heads_here + jnp.arange(heads_here, dtype=jnp.int32)
    slopes = jnp.exp2(-8.0 * (head_ids + 1).astype(jnp.float32) / QH).reshape(key_heads, groups)
    query_pos = jnp.arange(WINDOW, dtype=jnp.int32)
    key_pos = jnp.arange(2 * WINDOW, dtype=jnp.int32)
    distance = query_pos[:, None] - key_pos[None, :] + WINDOW
    start_pos = (
        lax.axis_index("sp") * stream_extent + (jnp.arange(blocks, dtype=jnp.int32) - 1) * WINDOW
    )
    absolute = start_pos[:, None] + key_pos[None, :]
    allowed = ((distance >= 0) & (distance < WINDOW))[None] & (absolute >= 0)[:, None, :]
    biased = scores - slopes[:, :, None, None, None] * distance.astype(jnp.float32)
    weights = jnp.where(allowed, jnp.exp(biased), 0.0)
    denominator = (
        jnp.sum(weights, axis=-1, keepdims=True)
        + jnp.exp(head_sink_logit.reshape(key_heads, groups))[:, :, None, None, None]
    )
    attention = (weights / denominator).astype(jnp.bfloat16)
    attended = jnp.einsum(
        "hgnqk,nkhd->nqhgd", attention, value_band, preferred_element_type=jnp.float32
    )
    return attended.reshape(stream_extent, heads_here * HD).astype(jnp.bfloat16)


def linear_attention(
    gated_query, gated_keys, gated_values, fading_exponent, linear_head_gain, starting_state
):
    stream_extent = gated_query.shape[0]
    head_total = gated_query.shape[1] // LOOKUP_FEATURES
    span_count = stream_extent // SPAN
    scaled_query = gated_query.astype(jnp.float32).reshape(
        span_count, SPAN, head_total, LOOKUP_FEATURES
    ) * LOOKUP_FEATURES ** (-0.5)
    keys_wide = gated_keys.astype(jnp.float32).reshape(
        span_count, SPAN, head_total, LOOKUP_FEATURES
    )
    values_wide = gated_values.astype(jnp.float32).reshape(span_count, SPAN, head_total, DV)
    running = jnp.cumsum(
        fading_exponent.reshape(span_count, SPAN, head_total, LOOKUP_FEATURES), axis=1
    )
    span_end = running[:, -1]
    query_with_decay = scaled_query * jnp.exp(running)
    inverse_keys = keys_wide * jnp.exp(-running)
    ending_keys = keys_wide * jnp.exp(span_end[:, None] - running)
    inner = jnp.einsum("nchk,nshk->nhcs", query_with_decay, inverse_keys, precision=HIGH_PRECISION)
    lower = jnp.tril(jnp.ones((SPAN, SPAN), dtype=bool))
    inner = jnp.where(lower, inner, 0.0)
    within = jnp.einsum("nhcs,nshv->nchv", inner, values_wide, precision=HIGH_PRECISION)

    def advance(running_state, inputs):
        query_portion, key_portion, value_portion, scale_factor = inputs
        layer_output = jnp.einsum(
            "fmy,mys->fms", query_portion, running_state, precision=HIGH_PRECISION
        )
        running_state = running_state * scale_factor[..., None] + jnp.einsum(
            "gxp,gxz->xpz", key_portion, value_portion, precision=HIGH_PRECISION
        )
        return (running_state, layer_output)

    start_state = jnp.zeros((head_total, LOOKUP_FEATURES, DV), jnp.float32)
    state_end, carried = lax.scan(
        advance, start_state, (query_with_decay, ending_keys, values_wide, jnp.exp(span_end))
    )
    device_decay = jnp.exp(jnp.sum(span_end, axis=0))
    prefix_sums = jnp.cumsum(span_end, axis=0) - span_end

    def combine(earlier, later):
        return (earlier[0] * later[0], later[0][..., None] * earlier[1] + later[1])

    decay_before, state_before = prefix(
        (device_decay, state_end),
        "sp",
        combine,
        (jnp.ones_like(device_decay), jnp.zeros_like(state_end)),
    )
    incoming_rows = state_before + decay_before[..., None] * starting_state
    crossing = jnp.einsum(
        "qwso,soz->qwsz",
        query_with_decay * jnp.exp(prefix_sums)[:, None],
        incoming_rows,
        precision=HIGH_PRECISION,
    )
    flat = (within + carried + crossing).reshape(stream_extent, head_total, DV)
    normal = (
        flat * lax.rsqrt(jnp.mean(flat * flat, axis=-1, keepdims=True) + EPS) * linear_head_gain
    )
    return normal.reshape(stream_extent, head_total * DV).astype(jnp.bfloat16)


def local(
    activations,
    input_norm_gain,
    window_query_weight,
    window_key_weight,
    window_value_weight,
    linear_query_weight,
    linear_key_weight,
    linear_value_weight,
    decay_down_factor,
    decay_up_factor,
    decay_offset_bias,
    extra_fading_exponent,
    starting_state,
    head_sink_logit,
    linear_head_gain,
    window_output_weight,
    linear_output_weight,
):
    gathered = lax.all_gather(activations, "tp", axis=1, tiled=True)
    widened = gathered.astype(jnp.float32)
    normed = (
        widened
        * lax.rsqrt(jnp.mean(widened * widened, axis=1, keepdims=True) + EPS)
        * input_norm_gain
    ).astype(jnp.bfloat16)
    row_total = normed.shape[0]
    matrices = (
        window_query_weight,
        window_key_weight,
        window_value_weight,
        linear_query_weight,
        linear_key_weight,
        linear_value_weight,
    )
    segments = (
        lax.all_gather(matrices[0], "sp", axis=0, tiled=True),
        lax.all_gather(matrices[1], "sp", axis=0, tiled=True),
        lax.all_gather(matrices[2], "sp", axis=0, tiled=True),
        lax.all_gather(matrices[3], "sp", axis=0, tiled=True),
        lax.all_gather(matrices[4], "sp", axis=0, tiled=True),
        lax.all_gather(matrices[5], "sp", axis=0, tiled=True),
    )
    projected = tuple(
        (jnp.dot(normed, segment, preferred_element_type=jnp.float32) for segment in segments)
    )
    near_query, near_keys, near_values, gated_query, gated_keys, gated_values = [
        product.astype(jnp.bfloat16) for product in projected
    ]
    low_rank = jnp.dot(normed, decay_down_factor, preferred_element_type=jnp.float32).astype(
        jnp.bfloat16
    )
    attention_energies = (
        jnp.dot(low_rank, decay_up_factor, preferred_element_type=jnp.float32) + decay_offset_bias
    )
    head_total = extra_fading_exponent.shape[1]
    fading_exponent = (jax.nn.log_sigmoid(attention_energies) / FADING_SOFTNESS).reshape(
        row_total, head_total, LOOKUP_FEATURES
    ) + extra_fading_exponent[:, :, None]
    near_out = window_attention(near_query, near_keys, near_values, head_sink_logit)
    gated_out = linear_attention(
        gated_query, gated_keys, gated_values, fading_exponent, linear_head_gain, starting_state
    )
    window_full, linear_full = (
        lax.all_gather(window_output_weight, "sp", axis=1, tiled=True),
        lax.all_gather(linear_output_weight, "sp", axis=1, tiled=True),
    )
    return lax.psum_scatter(
        (
            jnp.dot(near_out, window_full, preferred_element_type=jnp.float32)
            + jnp.dot(gated_out, linear_full, preferred_element_type=jnp.float32)
        ).astype(jnp.bfloat16),
        "tp",
        scatter_dimension=0,
        tiled=True,
    )


def head_window(near_query, near_keys, near_values, head_sink_logit, first_head):
    stream_extent = near_query.shape[0]
    key_heads = near_keys.shape[1] // HD
    heads_here = near_query.shape[1] // HD
    groups = heads_here // key_heads
    blocks = stream_extent // WINDOW

    def banded(current):
        extended = jnp.concatenate(
            [jnp.zeros((WINDOW, current.shape[1]), current.dtype), current], axis=0
        )
        earlier = extended[:stream_extent].reshape(blocks, WINDOW, key_heads, HD)
        present = extended[WINDOW:].reshape(blocks, WINDOW, key_heads, HD)
        return jnp.concatenate([earlier, present], axis=1)

    key_band = banded(near_keys)
    value_band = banded(near_values)
    queries = near_query.reshape(blocks, WINDOW, key_heads, groups, HD)
    scores = jnp.einsum(
        "nqhgd,nkhd->hgnqk", queries, key_band, preferred_element_type=jnp.float32
    ) * HD ** (-0.5)
    head_ids = first_head + jnp.arange(heads_here, dtype=jnp.int32)
    slopes = jnp.exp2(-8.0 * (head_ids + 1).astype(jnp.float32) / QH).reshape(key_heads, groups)
    query_pos = jnp.arange(WINDOW, dtype=jnp.int32)
    key_pos = jnp.arange(2 * WINDOW, dtype=jnp.int32)
    distance = query_pos[:, None] - key_pos[None, :] + WINDOW
    absolute = (jnp.arange(blocks, dtype=jnp.int32) - 1)[:, None] * WINDOW + key_pos[None, :]
    allowed = ((distance >= 0) & (distance < WINDOW))[None] & (absolute >= 0)[:, None, :]
    biased = scores - slopes[:, :, None, None, None] * distance.astype(jnp.float32)
    weights = jnp.where(allowed, jnp.exp(biased), 0.0)
    denominator = (
        jnp.sum(weights, axis=-1, keepdims=True)
        + jnp.exp(head_sink_logit.reshape(key_heads, groups))[:, :, None, None, None]
    )
    attention = (weights / denominator).astype(jnp.bfloat16)
    attended = jnp.einsum(
        "hgnqk,nkhd->nqhgd", attention, value_band, preferred_element_type=jnp.float32
    )
    return attended.reshape(stream_extent, heads_here * HD).astype(jnp.bfloat16)


def head_linear(gated_query, gated_keys, gated_values, fading, gain, state):
    stream_extent = gated_query.shape[0]
    heads = gated_query.shape[1] // LOOKUP_FEATURES
    spans = stream_extent // SPAN
    bf = jnp.bfloat16

    def mm(spec, a, b):
        return jnp.einsum(spec, a.astype(bf), b.astype(bf), preferred_element_type=jnp.float32)

    queries = gated_query.astype(jnp.float32).reshape(
        spans, SPAN, heads, LOOKUP_FEATURES
    ) * LOOKUP_FEATURES ** (-0.5)
    keys = gated_keys.astype(jnp.float32).reshape(spans, SPAN, heads, LOOKUP_FEATURES)
    values = gated_values.reshape(spans, SPAN, heads, DV)
    running = jnp.cumsum(fading.reshape(spans, SPAN, heads, LOOKUP_FEATURES), axis=1)
    span_end = running[:, -1]
    decayed = queries * jnp.exp(running)
    inner = mm("nchk,nshk->nhcs", decayed, keys * jnp.exp(-running))
    inner = jnp.where(jnp.tril(jnp.ones((SPAN, SPAN), dtype=bool)), inner, 0.0)
    within = mm("nhcs,nshv->nchv", inner, values)
    added = mm("nshk,nshv->nhkv", keys * jnp.exp(span_end[:, None] - running), values)
    scale = jnp.exp(span_end)
    before = []
    for n in range(spans):
        before.append(state)
        state = state * scale[n][..., None] + added[n]
    carried = mm("nchk,nhkv->nchv", decayed, jnp.stack(before))
    flat = within + carried
    normal = flat * lax.rsqrt(jnp.mean(flat * flat, axis=-1, keepdims=True) + EPS) * gain
    return normal.reshape(stream_extent, heads * DV).astype(bf)


MESH = pl.DeviceIdType.MESH
BF = jnp.bfloat16
F32 = jnp.float32


def dot(a, b):
    return jnp.dot(a, b, preferred_element_type=F32)


def remote(src, dst, send_sem, recv_sem, **where):
    return pltpu.make_async_remote_copy(
        src_ref=src,
        dst_ref=dst,
        send_sem=send_sem,
        recv_sem=recv_sem,
        device_id=where,
        device_id_type=MESH,
    )


def greet(sp, tp):
    s, t = lax.axis_index("sp"), lax.axis_index("tp")
    barrier = pltpu.get_barrier_semaphore()
    for ds in range(sp):
        for dt in range(tp):
            if ds or dt:
                where = {"sp": lax.rem(s + ds, sp), "tp": lax.rem(t + dt, tp)}
                pl.semaphore_signal(barrier, inc=1, device_id=where, device_id_type=MESH)
    pl.semaphore_wait(barrier, sp * tp - 1)


def project_kernel(sp, tp, widths, *refs):
    x, gain, down, fade = refs[:4]
    sources = refs[4:10]
    joined, small = refs[10:12]
    weights = refs[12:18]
    squares, normed, blocks, note, part, right_in, left_in = refs[18:25]
    w_sem, sq_sem, a_send, a_recv, f_send, l_sem, n_send, n_recv = refs[25:33]
    r_send, r_recv, b_send, b_recv = refs[33:37]
    s, t = lax.axis_index("sp"), lax.axis_index("tp")
    other = 1 - t
    per_half = sp // tp
    rows, half = x.shape
    width = half // per_half
    loads = [
        pltpu.make_async_copy(a, b, w_sem.at[i]) for i, (a, b) in enumerate(zip(sources, weights))
    ]
    for load in loads:
        load.start()
    wide = x[...].astype(F32)
    own = jnp.sum(wide * wide, axis=1, keepdims=True)
    squares[0] = jnp.broadcast_to(own, (rows, 128))
    greet(sp, tp)
    swap = remote(squares.at[0], squares.at[1], sq_sem.at[0], sq_sem.at[1], tp=other)
    swap.start()
    swap.wait()
    total = own + squares[1][:, :1]
    scale = lax.rsqrt(total / (half * tp) + EPS)
    for i in range(per_half):
        cols = slice(i * width, (i + 1) * width)
        normed[i] = (x[:, cols].astype(F32) * scale * gain[t, :, cols]).astype(BF)
    home = lax.div(s, per_half) == t

    def slice_send(i):
        j = t * per_half + i
        return remote(normed.at[i], blocks.at[s], a_send.at[i], a_recv.at[s], sp=j)

    for i in range(per_half):

        @pl.when(t * per_half + i != s)
        def _():
            slice_send(i).start()

        @pl.when(t * per_half + i == s)
        def _():
            keep = pltpu.make_async_copy(normed.at[i], blocks.at[s], l_sem)
            keep.start()
            keep.wait()

    low = jnp.zeros((down.shape[1], rows), F32)
    for i in range(per_half):
        low += lax.dot_general(
            down[t, :, i * width : (i + 1) * width],
            normed[i],
            (((1,), (1,)), ((), ())),
            preferred_element_type=F32,
        )
    note[s, t, : down.shape[1]] = low
    note[s, t, down.shape[1] :] = fade[...]

    def note_send(n):
        where = {"sp": lax.rem(s + n // tp, sp), "tp": lax.rem(t + n % tp, tp)}
        return remote(note.at[s, t], note.at[s, t], n_send.at[n], n_recv.at[s, t], **where)

    for n in range(1, sp * tp):
        note_send(n).start()
    for load in loads:
        load.wait()

    def forward(b):
        return remote(blocks.at[b], blocks.at[b], f_send.at[b], a_recv.at[b], tp=other)

    def right(b, d):
        return remote(
            part.at[b, d], right_in.at[b, d], r_send.at[b, d], r_recv.at[b, d], sp=jnp.minimum(s + 1, sp - 1)
        )

    def left(b, d):
        return remote(
            part.at[b, d], left_in.at[b, d], b_send.at[b, d], b_recv.at[b, d], sp=jnp.maximum(s - 1, 0)
        )

    def compute(k, carry):
        step = jnp.where(s < (sp + 1) // 2, k, sp - k)
        b = lax.rem(s + step, sp)

        @pl.when(jnp.logical_or(jnp.logical_not(home), b != s))
        def _():
            forward(b).wait_recv()

        @pl.when(home)
        def _():
            forward(b).start()

        block = blocks[b]
        keys = dot(block, weights[1][...])
        vals = dot(block, weights[2][...])

        def fill(d):
            at = 0
            for i, m in enumerate(weights):
                w = widths[i]
                if i == 1:
                    piece = keys[:, d * w : (d + 1) * w]
                elif i == 2:
                    piece = vals[:, d * w : (d + 1) * w]
                else:
                    piece = dot(block, m[:, d * w : (d + 1) * w])
                part[b, d, :, at : at + w] = piece.astype(BF)
                at += w

        for n in range(sp):
            fill(n)

        @pl.when(s == 0)
        def _():
            for d in range(sp - 1, 0, -1):
                right(b, d).start()

        @pl.when(s == sp - 1)
        def _():
            for d in range(sp - 1):
                left(b, d).start()

        return carry

    lax.fori_loop(0, sp, compute, 0)

    def relay(k, carry):
        br, bl = k, sp - 1 - k
        for n in range(sp - 1):
            dr, dl = sp - 1 - n, n

            @pl.when(jnp.logical_and(s > 0, s < dr))
            def _():
                right(br, dr).wait_recv()
                part[br, dr] = (part[br, dr].astype(F32) + right_in[br, dr].astype(F32)).astype(BF)
                right(br, dr).start()

            @pl.when(jnp.logical_and(s < sp - 1, s > dl))
            def _():
                left(bl, dl).wait_recv()
                part[bl, dl] = (part[bl, dl].astype(F32) + left_in[bl, dl].astype(F32)).astype(BF)
                left(bl, dl).start()

        return carry

    lax.fori_loop(0, sp, relay, 0)

    def finish(b, carry):
        joined[b] = part[b, s]

        @pl.when(s > 0)
        def _():
            right(b, s).wait_recv()
            joined[b] = (joined[b].astype(F32) + right_in[b, s].astype(F32)).astype(BF)

        @pl.when(s < sp - 1)
        def _():
            left(b, s).wait_recv()
            joined[b] = (joined[b].astype(F32) + left_in[b, s].astype(F32)).astype(BF)

        for d in range(sp):

            @pl.when(s < d)
            def _():
                right(b, d).wait_send()

            @pl.when(s > d)
            def _():
                left(b, d).wait_send()

        @pl.when(home)
        def _():
            forward(b).wait_send()

        return carry

    lax.fori_loop(0, sp, finish, 0)
    for i in range(per_half):

        @pl.when(t * per_half + i != s)
        def _():
            slice_send(i).wait_send()

    for n in range(1, sp * tp):
        note_send(n).wait_send()
        ps, pt = lax.rem(s + n // tp, sp), lax.rem(t + n % tp, tp)
        remote(note.at[ps, pt], note.at[ps, pt], n_send.at[n], n_recv.at[ps, pt], tp=other).wait_recv()
    small[...] = note[...]


def output_kernel(sp, tp, order, *refs):
    near, gated, near_w, gated_w, out = refs[:5]
    w1, w2, held, term, away, landed = refs[5:11]
    w_sem, r_send, r_recv, b_send, b_recv, t_send, t_recv, o_send, o_recv = refs[11:20]
    s, t = lax.axis_index("sp"), lax.axis_index("tp")
    other = 1 - t
    rows = held.shape[2]
    split = near.shape[1]
    part = rows // tp
    loads = [
        pltpu.make_async_copy(near_w, w1, w_sem.at[0]),
        pltpu.make_async_copy(gated_w, w2, w_sem.at[1]),
    ]
    for load in loads:
        load.start()
    for b in range(sp):
        held[b, s, :, :split] = near[b * rows : (b + 1) * rows]
        held[b, s, :, split:] = gated[b * rows : (b + 1) * rows]
    greet(sp, tp)

    def right(b, src):
        ref = held.at[b, src]
        return remote(ref, ref, r_send.at[b, src], r_recv.at[b, src], sp=jnp.minimum(s + 1, sp - 1))

    def left(b, src):
        ref = held.at[b, src]
        return remote(ref, ref, b_send.at[b, src], b_recv.at[b, src], sp=jnp.maximum(s - 1, 0))

    def start_own(b):
        @pl.when(s < sp - 1)
        def _():
            right(b, s).start()

        @pl.when(s > 0)
        def _():
            left(b, s).start()

    def swap(b):
        return remote(term.at[b, other], away.at[b], t_send.at[b], t_recv.at[b], tp=other)

    def deliver(b):
        return remote(term.at[b, t], landed.at[s], o_send.at[b], o_recv.at[s], sp=b)

    def close(b):
        swap(b).wait()
        term[b, t] = (term[b, t].astype(F32) + away[b].astype(F32)).astype(BF)

        @pl.when(s != b)
        def _():
            deliver(b).start()

        @pl.when(s == b)
        def _():
            landed[b] = term[b, t]

    start_own(order[0])
    for load in loads:
        load.wait()
    for k, b in enumerate(order):
        if k + 1 < sp:
            start_own(order[k + 1])
        for n in range(1, sp):

            @pl.when(s - n >= 0)
            def _():
                src = jnp.maximum(s - n, 0)
                right(b, src).wait_recv()

                @pl.when(s < sp - 1)
                def _():
                    right(b, src).start()

            @pl.when(s + n < sp)
            def _():
                src = jnp.minimum(s + n, sp - 1)
                left(b, src).wait_recv()

                @pl.when(s > 0)
                def _():
                    left(b, src).start()

        if k:
            close(order[k - 1])
        total = None
        for src in range(sp):
            block = held[b, src]
            piece = dot(block[:, :split], w1[src * split : (src + 1) * split]) + dot(
                block[:, split:], w2[src * (block.shape[1] - split) : (src + 1) * (block.shape[1] - split)]
            )
            total = piece if total is None else total + piece
        for h in range(tp):
            term[b, h] = total[h * part : (h + 1) * part].astype(BF)
        swap(b).start()
    close(order[-1])
    for b in range(sp):
        for src in range(sp):

            @pl.when(jnp.logical_and(src <= s, s < sp - 1))
            def _():
                right(b, src).wait_send()

            @pl.when(jnp.logical_and(src >= s, s > 0))
            def _():
                left(b, src).wait_send()

    for b in range(sp):

        @pl.when(s != b)
        def _():
            deliver(b).wait_send()
            remote(landed.at[b], landed.at[b], o_send.at[b], o_recv.at[b], tp=other).wait_recv()

    columns = landed.shape[2]
    for b in range(sp):
        out[:, b * columns : (b + 1) * columns] = landed[b]


def stationary(
    activations,
    input_norm_gain,
    window_query_weight,
    window_key_weight,
    window_value_weight,
    linear_query_weight,
    linear_key_weight,
    linear_value_weight,
    decay_down_factor,
    decay_up_factor,
    decay_offset_bias,
    extra_fading_exponent,
    starting_state,
    head_sink_logit,
    linear_head_gain,
    window_output_weight,
    linear_output_weight,
):
    sp, tp = lax.axis_size("sp"), lax.axis_size("tp")
    me_sp, me_tp = lax.axis_index("sp"), lax.axis_index("tp")
    rows, half = activations.shape
    tokens = rows * sp
    matrices = (
        window_query_weight,
        window_key_weight,
        window_value_weight,
        linear_query_weight,
        linear_key_weight,
        linear_value_weight,
    )
    widths = tuple(m.shape[1] // sp for m in matrices)
    total = sum(widths)
    rank = decay_down_factor.shape[1]
    heads_tp = extra_fading_exponent.shape[1]
    gain = input_norm_gain.reshape(tp, 1, half)
    down = decay_down_factor.T.reshape(rank, tp, half).transpose(1, 0, 2)
    fade = jnp.pad(extra_fading_exponent.T, ((0, -heads_tp % 8), (0, 0)))
    noted = rank + fade.shape[0]
    vmem = pl.BlockSpec(memory_space=pltpu.VMEM)
    anywhere = pl.BlockSpec(memory_space=pl.ANY)
    dma = pltpu.SemaphoreType.DMA
    joined, small = pl.pallas_call(
        functools.partial(project_kernel, sp, tp, widths),
        out_shape=(
            jax.ShapeDtypeStruct((sp, rows, total), BF),
            jax.ShapeDtypeStruct((sp, tp, noted, rows), F32),
        ),
        in_specs=[vmem] * 4 + [anywhere] * 6,
        out_specs=(vmem, vmem),
        scratch_shapes=[pltpu.VMEM(m.shape, BF) for m in matrices]
        + [
            pltpu.VMEM((2, rows, 128), F32),
            pltpu.VMEM((sp // tp, rows, half * tp // sp), BF),
            pltpu.VMEM((sp, rows, half * tp // sp), BF),
            pltpu.VMEM((sp, tp, noted, rows), F32),
            pltpu.VMEM((sp, sp, rows, total), BF),
            pltpu.VMEM((sp, sp, rows, total), BF),
            pltpu.VMEM((sp, sp, rows, total), BF),
            dma((6,)),
            dma((2,)),
            dma((sp // tp,)),
            dma((sp,)),
            dma((sp,)),
            dma,
            dma((sp * tp,)),
            dma((sp, tp)),
            dma((sp, sp)),
            dma((sp, sp)),
            dma((sp, sp)),
            dma((sp, sp)),
        ],
        compiler_params=pltpu.CompilerParams(
            collective_id=0, has_side_effects=True, vmem_limit_bytes=48 * 2**20
        ),
    )(activations, gain, down, fade, *matrices)
    joined = joined.reshape(tokens, total)
    low_rank = (
        jnp.sum(small[:, :, :rank], axis=1).transpose(0, 2, 1).reshape(tokens, rank).astype(BF)
    )
    heads = heads_tp // sp
    fade_own = lax.dynamic_slice_in_dim(
        lax.dynamic_index_in_dim(small, me_tp, 1, False), rank + me_sp * heads, heads, 1
    )
    fade_own = fade_own.transpose(0, 2, 1).reshape(tokens, heads)
    pieces, at = [], 0
    for width in widths:
        pieces.append(joined[:, at : at + width])
        at += width
    near_query, near_keys, near_values, gated_query, gated_keys, gated_values = pieces
    channels = heads * LOOKUP_FEATURES
    up = lax.dynamic_slice_in_dim(decay_up_factor, me_sp * channels, channels, 1)
    bias = lax.dynamic_slice_in_dim(decay_offset_bias, me_sp * channels, channels, 0)
    energies = jnp.dot(low_rank, up, preferred_element_type=jnp.float32) + bias
    fading = (jax.nn.log_sigmoid(energies) / FADING_SOFTNESS).reshape(
        tokens, heads, LOOKUP_FEATURES
    ) + fade_own[:, :, None]
    near_heads = near_query.shape[1] // HD
    sinks = lax.dynamic_slice_in_dim(head_sink_logit, me_sp * near_heads, near_heads, 0)
    near_out = head_window(
        near_query, near_keys, near_values, sinks, (me_tp * sp + me_sp) * near_heads
    )
    state = lax.dynamic_slice_in_dim(starting_state, me_sp * heads, heads, 0)
    gated_out = head_linear(
        gated_query, gated_keys, gated_values, fading, linear_head_gain, state
    )
    columns = window_output_weight.shape[1]
    both = near_out.shape[1] + gated_out.shape[1]
    order = sorted(range(sp), key=lambda b: -abs(2 * b - sp + 1))
    return pl.pallas_call(
        functools.partial(output_kernel, sp, tp, order),
        out_shape=jax.ShapeDtypeStruct((rows // tp, columns * sp), BF),
        in_specs=[vmem] * 2 + [anywhere] * 2,
        out_specs=vmem,
        scratch_shapes=[
            pltpu.VMEM(window_output_weight.shape, BF),
            pltpu.VMEM(linear_output_weight.shape, BF),
            pltpu.VMEM((sp, sp, rows, both), BF),
            pltpu.VMEM((sp, tp, rows // tp, columns), BF),
            pltpu.VMEM((sp, rows // tp, columns), BF),
            pltpu.VMEM((sp, rows // tp, columns), BF),
            dma((2,)),
            dma((sp, sp)),
            dma((sp, sp)),
            dma((sp, sp)),
            dma((sp, sp)),
            dma((sp,)),
            dma((sp,)),
            dma((sp,)),
            dma((sp,)),
        ],
        compiler_params=pltpu.CompilerParams(
            collective_id=1, has_side_effects=True, vmem_limit_bytes=48 * 2**20
        ),
    )(near_out, gated_out, window_output_weight, linear_output_weight)


def divides(sp, tp):
    heads = sp * tp
    fits = GATED_MIXERS % heads == 0 and KVH % heads == 0 and QH % heads == 0
    return tp == 2 and sp % tp == 0 and fits


def solution(mesh):
    placed = (
        P(("fs", "sp"), "tp"),
        P(),
        P("sp", "tp"),
        P("sp", "tp"),
        P("sp", "tp"),
        P("sp", "tp"),
        P("sp", "tp"),
        P("sp", "tp"),
        P(),
        P(None, "tp"),
        P("tp"),
        P(("fs", "sp"), "tp"),
        P("tp", None, None),
        P("tp"),
        P(),
        P("tp", "sp"),
        P("tp", "sp"),
    )
    body = stationary if divides(mesh.shape["sp"], mesh.shape["tp"]) else local
    return jax.shard_map(
        body, mesh=mesh, in_specs=placed, out_specs=P(("fs", "sp", "tp"), None), check_vma=False
    )
```

```python
import functools

import jax
import jax.numpy as jnp
from jax import lax
from jax.experimental import pallas as pl
from jax.experimental.pallas import tpu as pltpu
from jax.sharding import PartitionSpec as P

QH = 32
HD = 64
WINDOW = 128
LOOKUP_FEATURES = 128
DV = 256
SPAN = 64
KVH = 8
GATED_MIXERS = 8


EPS = 1e-05
FADING_SOFTNESS = 16.0
HIGH_PRECISION = lax.Precision.HIGHEST


def passed_along(value, axis, steps):
    count = lax.axis_size(axis)
    leading, last = (max(0, -steps), min(count, count - steps))
    return lax.ppermute(value, axis, [(source, source + steps) for source in range(leading, last)])


def prefix(x, axis, combine, identity):
    peers, place = (lax.axis_size(axis), lax.axis_index(axis))
    everything = jax.tree.map(
        lambda part, kind: lax.all_gather(part.astype(kind), axis), x, (jnp.bfloat16, jnp.bfloat16)
    )
    start = jax.tree.map(
        lambda part, zero: jnp.broadcast_to(jnp.asarray(zero, part.dtype), part.shape), x, identity
    )

    def hop(k, before):
        reached = k < place
        new = combine(
            before, jax.tree.map(lambda part, own: part[k].astype(own.dtype), everything, x)
        )
        return jax.tree.map(lambda a, b: jnp.where(reached, a, b), new, before)

    return lax.fori_loop(0, peers, hop, start)


def window_attention(near_query, near_keys, near_values, head_sink_logit):
    stream_extent = near_query.shape[0]
    key_heads = near_keys.shape[1] // HD
    heads_here = near_query.shape[1] // HD
    groups = heads_here // key_heads
    blocks = stream_extent // WINDOW
    tail_rows = jnp.stack([near_keys, near_values])
    before = passed_along(tail_rows, "sp", 1)

    def banded(previous, current):
        extended = jnp.concatenate([previous, current], axis=0)
        earlier = extended[:stream_extent].reshape(blocks, WINDOW, key_heads, HD)
        present = extended[WINDOW:].reshape(blocks, WINDOW, key_heads, HD)
        return jnp.concatenate([earlier, present], axis=1)

    key_band = banded(before[0], near_keys)
    value_band = banded(before[1], near_values)
    queries = near_query.reshape(blocks, WINDOW, key_heads, groups, HD)
    scores = jnp.einsum(
        "nqhgd,nkhd->hgnqk", queries, key_band, preferred_element_type=jnp.float32
    ) * HD ** (-0.5)
    head_ids = lax.axis_index("tp") * heads_here + jnp.arange(heads_here, dtype=jnp.int32)
    slopes = jnp.exp2(-8.0 * (head_ids + 1).astype(jnp.float32) / QH).reshape(key_heads, groups)
    query_pos = jnp.arange(WINDOW, dtype=jnp.int32)
    key_pos = jnp.arange(2 * WINDOW, dtype=jnp.int32)
    distance = query_pos[:, None] - key_pos[None, :] + WINDOW
    start_pos = (
        lax.axis_index("sp") * stream_extent + (jnp.arange(blocks, dtype=jnp.int32) - 1) * WINDOW
    )
    absolute = start_pos[:, None] + key_pos[None, :]
    allowed = ((distance >= 0) & (distance < WINDOW))[None] & (absolute >= 0)[:, None, :]
    biased = scores - slopes[:, :, None, None, None] * distance.astype(jnp.float32)
    weights = jnp.where(allowed, jnp.exp(biased), 0.0)
    denominator = (
        jnp.sum(weights, axis=-1, keepdims=True)
        + jnp.exp(head_sink_logit.reshape(key_heads, groups))[:, :, None, None, None]
    )
    attention = (weights / denominator).astype(jnp.bfloat16)
    attended = jnp.einsum(
        "hgnqk,nkhd->nqhgd", attention, value_band, preferred_element_type=jnp.float32
    )
    return attended.reshape(stream_extent, heads_here * HD).astype(jnp.bfloat16)


def linear_attention(
    gated_query, gated_keys, gated_values, fading_exponent, linear_head_gain, starting_state
):
    stream_extent = gated_query.shape[0]
    head_total = gated_query.shape[1] // LOOKUP_FEATURES
    span_count = stream_extent // SPAN
    scaled_query = gated_query.astype(jnp.float32).reshape(
        span_count, SPAN, head_total, LOOKUP_FEATURES
    ) * LOOKUP_FEATURES ** (-0.5)
    keys_wide = gated_keys.astype(jnp.float32).reshape(
        span_count, SPAN, head_total, LOOKUP_FEATURES
    )
    values_wide = gated_values.astype(jnp.float32).reshape(span_count, SPAN, head_total, DV)
    running = jnp.cumsum(
        fading_exponent.reshape(span_count, SPAN, head_total, LOOKUP_FEATURES), axis=1
    )
    span_end = running[:, -1]
    query_with_decay = scaled_query * jnp.exp(running)
    inverse_keys = keys_wide * jnp.exp(-running)
    ending_keys = keys_wide * jnp.exp(span_end[:, None] - running)
    inner = jnp.einsum("nchk,nshk->nhcs", query_with_decay, inverse_keys, precision=HIGH_PRECISION)
    lower = jnp.tril(jnp.ones((SPAN, SPAN), dtype=bool))
    inner = jnp.where(lower, inner, 0.0)
    within = jnp.einsum("nhcs,nshv->nchv", inner, values_wide, precision=HIGH_PRECISION)

    def advance(running_state, inputs):
        query_portion, key_portion, value_portion, scale_factor = inputs
        layer_output = jnp.einsum(
            "fmy,mys->fms", query_portion, running_state, precision=HIGH_PRECISION
        )
        running_state = running_state * scale_factor[..., None] + jnp.einsum(
            "gxp,gxz->xpz", key_portion, value_portion, precision=HIGH_PRECISION
        )
        return (running_state, layer_output)

    start_state = jnp.zeros((head_total, LOOKUP_FEATURES, DV), jnp.float32)
    state_end, carried = lax.scan(
        advance, start_state, (query_with_decay, ending_keys, values_wide, jnp.exp(span_end))
    )
    device_decay = jnp.exp(jnp.sum(span_end, axis=0))
    prefix_sums = jnp.cumsum(span_end, axis=0) - span_end

    def combine(earlier, later):
        return (earlier[0] * later[0], later[0][..., None] * earlier[1] + later[1])

    decay_before, state_before = prefix(
        (device_decay, state_end),
        "sp",
        combine,
        (jnp.ones_like(device_decay), jnp.zeros_like(state_end)),
    )
    incoming_rows = state_before + decay_before[..., None] * starting_state
    crossing = jnp.einsum(
        "qwso,soz->qwsz",
        query_with_decay * jnp.exp(prefix_sums)[:, None],
        incoming_rows,
        precision=HIGH_PRECISION,
    )
    flat = (within + carried + crossing).reshape(stream_extent, head_total, DV)
    normal = (
        flat * lax.rsqrt(jnp.mean(flat * flat, axis=-1, keepdims=True) + EPS) * linear_head_gain
    )
    return normal.reshape(stream_extent, head_total * DV).astype(jnp.bfloat16)


def local(
    activations,
    input_norm_gain,
    window_query_weight,
    window_key_weight,
    window_value_weight,
    linear_query_weight,
    linear_key_weight,
    linear_value_weight,
    decay_down_factor,
    decay_up_factor,
    decay_offset_bias,
    extra_fading_exponent,
    starting_state,
    head_sink_logit,
    linear_head_gain,
    window_output_weight,
    linear_output_weight,
):
    gathered = lax.all_gather(activations, "tp", axis=1, tiled=True)
    widened = gathered.astype(jnp.float32)
    normed = (
        widened
        * lax.rsqrt(jnp.mean(widened * widened, axis=1, keepdims=True) + EPS)
        * input_norm_gain
    ).astype(jnp.bfloat16)
    row_total = normed.shape[0]
    matrices = (
        window_query_weight,
        window_key_weight,
        window_value_weight,
        linear_query_weight,
        linear_key_weight,
        linear_value_weight,
    )
    segments = (
        lax.all_gather(matrices[0], "sp", axis=0, tiled=True),
        lax.all_gather(matrices[1], "sp", axis=0, tiled=True),
        lax.all_gather(matrices[2], "sp", axis=0, tiled=True),
        lax.all_gather(matrices[3], "sp", axis=0, tiled=True),
        lax.all_gather(matrices[4], "sp", axis=0, tiled=True),
        lax.all_gather(matrices[5], "sp", axis=0, tiled=True),
    )
    projected = tuple(
        (jnp.dot(normed, segment, preferred_element_type=jnp.float32) for segment in segments)
    )
    near_query, near_keys, near_values, gated_query, gated_keys, gated_values = [
        product.astype(jnp.bfloat16) for product in projected
    ]
    low_rank = jnp.dot(normed, decay_down_factor, preferred_element_type=jnp.float32).astype(
        jnp.bfloat16
    )
    attention_energies = (
        jnp.dot(low_rank, decay_up_factor, preferred_element_type=jnp.float32) + decay_offset_bias
    )
    head_total = extra_fading_exponent.shape[1]
    fading_exponent = (jax.nn.log_sigmoid(attention_energies) / FADING_SOFTNESS).reshape(
        row_total, head_total, LOOKUP_FEATURES
    ) + extra_fading_exponent[:, :, None]
    near_out = window_attention(near_query, near_keys, near_values, head_sink_logit)
    gated_out = linear_attention(
        gated_query, gated_keys, gated_values, fading_exponent, linear_head_gain, starting_state
    )
    window_full, linear_full = (
        lax.all_gather(window_output_weight, "sp", axis=1, tiled=True),
        lax.all_gather(linear_output_weight, "sp", axis=1, tiled=True),
    )
    return lax.psum_scatter(
        (
            jnp.dot(near_out, window_full, preferred_element_type=jnp.float32)
            + jnp.dot(gated_out, linear_full, preferred_element_type=jnp.float32)
        ).astype(jnp.bfloat16),
        "tp",
        scatter_dimension=0,
        tiled=True,
    )


MESH = pl.DeviceIdType.MESH
BF = jnp.bfloat16
F32 = jnp.float32


def dot(a, b):
    return jnp.dot(a, b, preferred_element_type=F32)


def remote(src, dst, send_sem, recv_sem, **where):
    return pltpu.make_async_remote_copy(
        src_ref=src,
        dst_ref=dst,
        send_sem=send_sem,
        recv_sem=recv_sem,
        device_id=where,
        device_id_type=MESH,
    )


def greet(sp, tp):
    s, t = lax.axis_index("sp"), lax.axis_index("tp")
    barrier = pltpu.get_barrier_semaphore()
    for ds in range(sp):
        for dt in range(tp):
            if ds or dt:
                where = {"sp": lax.rem(s + ds, sp), "tp": lax.rem(t + dt, tp)}
                pl.semaphore_signal(barrier, inc=1, device_id=where, device_id_type=MESH)
    pl.semaphore_wait(barrier, sp * tp - 1)


def columns_dot(a, b):
    return lax.dot_general(a, b, (((1,), (1,)), ((), ())), preferred_element_type=F32)


def mixer_kernel(sp, tp, widths, order, *refs):
    x, gain, down, fade, up, bias, sink, head_gain = refs[:8]
    sources, state_in, out = refs[8:16], refs[16], refs[17]
    weights, start = refs[18:26], refs[26]
    squares, normed, blocks, note, term, away, landed = refs[27:34]
    lin = refs[34:38]
    win = refs[38:42]
    held_g, held_n = refs[42:44]
    w_sem, sq_sem, a_send, a_recv, f_send, l_sem, n_send, n_recv = refs[44:52]
    lin_sem, win_sem, g_sem, h_sem = refs[52:56], refs[56:60], refs[60:64], refs[64:68]
    t_send, t_recv, o_send, o_recv = refs[68:72]
    s, t = lax.axis_index("sp"), lax.axis_index("tp")
    other = 1 - t
    after, ahead = jnp.minimum(s + 1, sp - 1), jnp.maximum(s - 1, 0)
    per_half = sp // tp
    rows, half = x.shape
    width = half // per_half
    rank = down.shape[1]
    loads = [
        pltpu.make_async_copy(a, b, w_sem.at[i]) for i, (a, b) in enumerate(zip(sources, weights))
    ]
    loads.append(pltpu.make_async_copy(state_in.at[s], start, w_sem.at[len(sources)]))
    for i in (3, 4, 5, 0, 1, 2, 8, 6, 7):
        loads[i].start()
    wide = x[...].astype(F32)
    own = jnp.sum(wide * wide, axis=1, keepdims=True)
    squares[0] = jnp.broadcast_to(own, (rows, 128))
    greet(sp, tp)
    swap_squares = remote(squares.at[0], squares.at[1], sq_sem.at[0], sq_sem.at[1], tp=other)
    swap_squares.start()
    swap_squares.wait()
    total = own + squares[1][:, :1]
    scale = lax.rsqrt(total / (half * tp) + EPS)
    home = lax.div(s, per_half) == t

    def slice_send(i):
        j = t * per_half + i
        return remote(normed.at[i], blocks.at[s], a_send.at[i], a_recv.at[s], sp=j)

    for i in range(per_half):
        cols = slice(i * width, (i + 1) * width)
        normed[i] = (x[:, cols].astype(F32) * scale * gain[t, :, cols]).astype(BF)

        @pl.when(t * per_half + i != s)
        def _():
            slice_send(i).start()

        @pl.when(t * per_half + i == s)
        def _():
            keep = pltpu.make_async_copy(normed.at[i], blocks.at[s], l_sem)
            keep.start()
            keep.wait()

    def forward(b):
        return remote(blocks.at[b], blocks.at[b], f_send.at[b], a_recv.at[b], tp=other)

    @pl.when(home)
    def _():
        forward(s).start()

    low = jnp.zeros((rank, rows), F32)
    for i in range(per_half):
        low += columns_dot(down[t, :, i * width : (i + 1) * width], normed[i])
    note[s, t, :rank] = low
    note[s, t, rank:] = fade[...]

    def note_send(n):
        where = {"sp": lax.rem(s + n // tp, sp), "tp": lax.rem(t + n % tp, tp)}
        return remote(note.at[s, t], note.at[s, t], n_send.at[n], n_recv.at[s, t], **where)

    def right(group, sems, b, d):
        return remote(group[0].at[b, d], group[1].at[b, d], sems[0].at[b, d], sems[1].at[b, d], sp=after)

    def left(group, sems, b, d):
        return remote(group[0].at[b, d], group[2].at[b, d], sems[2].at[b, d], sems[3].at[b, d], sp=ahead)

    def ends(group, sems, b):
        @pl.when(s == 0)
        def _():
            for d in range(sp - 1, 0, -1):
                right(group, sems, b, d).start()

        @pl.when(s == sp - 1)
        def _():
            for d in range(sp - 1):
                left(group, sems, b, d).start()

    def place(k):
        return lax.rem(s + jnp.where(s < (sp + 1) // 2, k, sp - k), sp)

    for i in (3, 4, 5):
        loads[i].wait()

    def project_linear(k, carry):
        b = place(k)

        @pl.when(jnp.logical_or(jnp.logical_not(home), b != s))
        def _():
            forward(b).wait_recv()

        @pl.when(jnp.logical_and(home, b != s))
        def _():
            forward(b).start()

        block = blocks[b]
        for d in range(sp):
            at = 0
            for i in (3, 4, 5):
                w = widths[i]
                lin[0][b, d, :, at : at + w] = dot(block, weights[i][:, d * w : (d + 1) * w]).astype(BF)
                at += w
        ends(lin, lin_sem, b)
        return carry

    lax.fori_loop(0, sp, project_linear, 0)
    for n in range(1, sp * tp):
        note_send(n).start()
    for i in (0, 1, 2):
        loads[i].wait()

    def relay(group, sems, k):
        br, bl = k, sp - 1 - k
        for n in range(sp - 1):
            dr, dl = sp - 1 - n, n

            @pl.when(jnp.logical_and(s > 0, s < dr))
            def _():
                right(group, sems, br, dr).wait_recv()
                group[0][br, dr] = (
                    group[0][br, dr].astype(F32) + group[1][br, dr].astype(F32)
                ).astype(BF)
                right(group, sems, br, dr).start()

            @pl.when(jnp.logical_and(s < sp - 1, s > dl))
            def _():
                left(group, sems, bl, dl).wait_recv()
                group[0][bl, dl] = (
                    group[0][bl, dl].astype(F32) + group[2][bl, dl].astype(F32)
                ).astype(BF)
                left(group, sems, bl, dl).start()

    def project_window(k, carry):
        b = place(k)
        block = blocks[b]
        keys = dot(block, weights[1][...])
        vals = dot(block, weights[2][...])
        qw, kw, vw = widths[:3]
        for d in range(sp):
            win[0][b, d, :, :qw] = dot(block, weights[0][:, d * qw : (d + 1) * qw]).astype(BF)
            win[0][b, d, :, qw : qw + kw] = keys[:, d * kw : (d + 1) * kw].astype(BF)
            win[0][b, d, :, qw + kw :] = vals[:, d * vw : (d + 1) * vw].astype(BF)
        ends(win, win_sem, b)
        relay(lin, lin_sem, k)
        return carry

    lax.fori_loop(0, sp, project_window, 0)

    def finish(group, sems, b):
        group[3][b] = group[0][b, s]

        @pl.when(s > 0)
        def _():
            right(group, sems, b, s).wait_recv()
            group[3][b] = (group[3][b].astype(F32) + group[1][b, s].astype(F32)).astype(BF)

        @pl.when(s < sp - 1)
        def _():
            left(group, sems, b, s).wait_recv()
            group[3][b] = (group[3][b].astype(F32) + group[2][b, s].astype(F32)).astype(BF)

    def sent(group, sems, b):
        for d in range(sp):

            @pl.when(s < d)
            def _():
                right(group, sems, b, d).wait_send()

            @pl.when(s > d)
            def _():
                left(group, sems, b, d).wait_send()

    def gather_right(held, sems, b, src):
        ref = held.at[b, src]
        return remote(ref, ref, sems[0].at[b, src], sems[1].at[b, src], sp=after)

    def gather_left(held, sems, b, src):
        ref = held.at[b, src]
        return remote(ref, ref, sems[2].at[b, src], sems[3].at[b, src], sp=ahead)

    def start_own(held, sems, b):
        @pl.when(s < sp - 1)
        def _():
            gather_right(held, sems, b, s).start()

        @pl.when(s > 0)
        def _():
            gather_left(held, sems, b, s).start()

    def pass_on(held, sems, b):
        for n in range(1, sp):

            @pl.when(s - n >= 0)
            def _():
                src = jnp.maximum(s - n, 0)
                gather_right(held, sems, b, src).wait_recv()

                @pl.when(s < sp - 1)
                def _():
                    gather_right(held, sems, b, src).start()

            @pl.when(s + n < sp)
            def _():
                src = jnp.minimum(s + n, sp - 1)
                gather_left(held, sems, b, src).wait_recv()

                @pl.when(s > 0)
                def _():
                    gather_left(held, sems, b, src).start()

    loads[8].wait()
    for n in range(1, sp * tp):
        ps, pt = lax.rem(s + n // tp, sp), lax.rem(t + n % tp, tp)
        remote(note.at[ps, pt], note.at[ps, pt], n_send.at[n], n_recv.at[ps, pt], tp=other).wait_recv()
    lk = LOOKUP_FEATURES
    lane = pl.ds(pl.multiple_of(s * lk, lk), lk)
    up_own = jnp.concatenate([up[:, lane], jnp.zeros((rows - rank, lk), BF)], axis=0)
    bias_own = bias[:, lane]
    row_at = lax.broadcasted_iota(jnp.int32, (rows, rows), 0)
    col_at = lax.broadcasted_iota(jnp.int32, (rows, rows), 1)
    span_low = jnp.logical_and(row_at >= col_at, row_at // SPAN == col_at // SPAN)
    ones_low = jnp.where(span_low, 1.0, 0.0)
    noted = note.shape[2]

    def linear(b, state):
        finish(lin, lin_sem, b)
        rank_rows = note[b, 0, :rank] + note[b, 1, :rank]
        tall = jnp.concatenate(
            [rank_rows, note[b, t, rank:], jnp.zeros((rows - noted, rows), F32)], axis=0
        ).T
        energies = dot(tall.astype(BF), up_own) + bias_own
        soft = jnp.minimum(energies, 0.0) - jnp.log1p(jnp.exp(-jnp.abs(energies)))
        extra = jnp.sum(jnp.where(col_at == rank + s, tall, 0.0), axis=1, keepdims=True)
        fading = soft / FADING_SOFTNESS + extra
        running = lax.dot_general(
            ones_low,
            fading,
            (((1,), (0,)), ((), ())),
            precision=HIGH_PRECISION,
            preferred_element_type=F32,
        )
        query = lin[3][b, :, :lk].astype(F32) * lk ** (-0.5)
        key = lin[3][b, :, lk : 2 * lk].astype(F32)
        value = lin[3][b, :, 2 * lk :]
        decayed = (query * jnp.exp(running)).astype(BF)
        inner = columns_dot(decayed, (key * jnp.exp(-running)).astype(BF))
        inner = jnp.where(span_low, inner, 0.0).astype(BF)
        within = dot(inner, value)
        carried = []
        for j in range(rows // SPAN):
            cut = slice(j * SPAN, (j + 1) * SPAN)
            end = running[(j + 1) * SPAN - 1 : (j + 1) * SPAN]
            ending = (key[cut] * jnp.exp(end - running[cut])).astype(BF)
            carried.append(columns_dot(decayed[cut], state.astype(BF)))
            state = state * jnp.exp(end) + lax.dot_general(
                value[cut], ending, (((0,), (0,)), ((), ())), preferred_element_type=F32
            )
        flat = within + jnp.concatenate(carried, axis=0)
        normal = flat * lax.rsqrt(jnp.mean(flat * flat, axis=-1, keepdims=True) + EPS) * head_gain[...]
        held_g[b, s] = normal.astype(BF)
        start_own(held_g, g_sem, b)
        return state

    lax.fori_loop(0, sp, linear, start[...].T)

    def relay_window(k, carry):
        relay(win, win_sem, k)
        pass_on(held_g, g_sem, k)
        return carry

    lax.fori_loop(0, sp, relay_window, 0)

    def finish_window(b, carry):
        finish(win, win_sem, b)
        return carry

    lax.fori_loop(0, sp, finish_window, 0)
    query_at = lax.broadcasted_iota(jnp.int32, (rows, 2 * rows), 0)
    key_at = lax.broadcasted_iota(jnp.int32, (rows, 2 * rows), 1)
    distance = query_at - key_at + rows
    near_by = jnp.logical_and(distance >= 0, distance < WINDOW)
    far = distance.astype(F32)
    heads = widths[0] // HD
    qw = widths[0]
    for b in order:
        present = win[3][b]
        earlier = win[3][max(b - 1, 0)]
        keys = jnp.concatenate([earlier[:, qw : qw + HD], present[:, qw : qw + HD]], axis=0)
        vals = jnp.concatenate([earlier[:, qw + HD :], present[:, qw + HD :]], axis=0)
        allowed = near_by if b else jnp.logical_and(near_by, key_at >= rows)
        results = []
        for h in range(heads):
            number = ((t * sp + s) * heads + h + 1).astype(F32)
            slope = jnp.exp2(jnp.full((rows, 1), -8.0 / QH, F32) * number)
            score = columns_dot(present[:, h * HD : (h + 1) * HD], keys) * HD ** (-0.5) - slope * far
            weight = jnp.where(allowed, jnp.exp(score), 0.0)
            floor = jnp.exp(jnp.full((rows, 1), sink[s * heads + h], F32))
            probs = (weight / (jnp.sum(weight, axis=1, keepdims=True) + floor)).astype(BF)
            results.append(dot(probs, vals))
        held_n[b, s] = jnp.concatenate(results, axis=1).astype(BF)
        start_own(held_n, h_sem, b)

    loads[6].wait()
    loads[7].wait()
    part = rows // tp
    near_cols, gated_cols = held_n.shape[3], held_g.shape[3]

    def swap(b):
        return remote(term.at[b, other], away.at[b], t_send.at[b], t_recv.at[b], tp=other)

    def deliver(b):
        return remote(term.at[b, t], landed.at[s], o_send.at[b], o_recv.at[s], sp=b)

    def close(b):
        swap(b).wait()
        term[b, t] = (term[b, t].astype(F32) + away[b].astype(F32)).astype(BF)

        @pl.when(s != b)
        def _():
            deliver(b).start()

        @pl.when(s == b)
        def _():
            landed[b] = term[b, t]

    for k, b in enumerate(order):
        pass_on(held_n, h_sem, b)
        if k:
            close(order[k - 1])
        total = None
        for src in range(sp):
            piece = dot(held_n[b, src], weights[6][src * near_cols : (src + 1) * near_cols]) + dot(
                held_g[b, src], weights[7][src * gated_cols : (src + 1) * gated_cols]
            )
            total = piece if total is None else total + piece
        for h in range(tp):
            term[b, h] = total[h * part : (h + 1) * part].astype(BF)
        swap(b).start()
    close(order[-1])

    def drain(b, carry):
        sent(lin, lin_sem, b)
        sent(win, win_sem, b)

        @pl.when(home)
        def _():
            forward(b).wait_send()

        for held, sems in ((held_g, g_sem), (held_n, h_sem)):
            for src in range(sp):

                @pl.when(jnp.logical_and(src <= s, s < sp - 1))
                def _():
                    gather_right(held, sems, b, src).wait_send()

                @pl.when(jnp.logical_and(src >= s, s > 0))
                def _():
                    gather_left(held, sems, b, src).wait_send()

        return carry

    lax.fori_loop(0, sp, drain, 0)
    for i in range(per_half):

        @pl.when(t * per_half + i != s)
        def _():
            slice_send(i).wait_send()

    for n in range(1, sp * tp):
        note_send(n).wait_send()
    columns = landed.shape[2]
    for b in range(sp):

        @pl.when(s != b)
        def _():
            deliver(b).wait_send()
            remote(landed.at[b], landed.at[b], o_send.at[b], o_recv.at[b], tp=other).wait_recv()

        out[:, b * columns : (b + 1) * columns] = landed[b]


def stationary(
    activations,
    input_norm_gain,
    window_query_weight,
    window_key_weight,
    window_value_weight,
    linear_query_weight,
    linear_key_weight,
    linear_value_weight,
    decay_down_factor,
    decay_up_factor,
    decay_offset_bias,
    extra_fading_exponent,
    starting_state,
    head_sink_logit,
    linear_head_gain,
    window_output_weight,
    linear_output_weight,
):
    sp, tp = lax.axis_size("sp"), lax.axis_size("tp")
    rows, half = activations.shape
    matrices = (
        window_query_weight,
        window_key_weight,
        window_value_weight,
        linear_query_weight,
        linear_key_weight,
        linear_value_weight,
        window_output_weight,
        linear_output_weight,
    )
    widths = tuple(m.shape[1] // sp for m in matrices[:6])
    wide_window, wide_linear = sum(widths[:3]), sum(widths[3:])
    rank = decay_down_factor.shape[1]
    heads_tp = extra_fading_exponent.shape[1]
    gain = input_norm_gain.reshape(tp, 1, half)
    down = decay_down_factor.T.reshape(rank, tp, half).transpose(1, 0, 2)
    fade = jnp.pad(extra_fading_exponent.T, ((0, -heads_tp % 8), (0, 0)))
    noted = rank + fade.shape[0]
    columns = window_output_weight.shape[1]
    order = sorted(range(sp), key=lambda b: -abs(2 * b - sp + 1))
    vmem = pl.BlockSpec(memory_space=pltpu.VMEM)
    hbm = pl.BlockSpec(memory_space=pltpu.HBM)
    dma = pltpu.SemaphoreType.DMA
    slice_width = half * tp // sp

    def chunks(cols):
        return [pltpu.VMEM((sp, sp, rows, cols), BF)] * 3 + [pltpu.VMEM((sp, rows, cols), BF)]

    return pl.pallas_call(
        functools.partial(mixer_kernel, sp, tp, widths, order),
        out_shape=jax.ShapeDtypeStruct((rows // tp, columns * sp), BF),
        in_specs=[vmem] * 6
        + [pl.BlockSpec(memory_space=pltpu.SMEM), vmem]
        + [hbm] * 9,
        out_specs=vmem,
        scratch_shapes=[pltpu.VMEM(m.shape, BF) for m in matrices]
        + [
            pltpu.VMEM(starting_state.shape[1:], F32),
            pltpu.VMEM((2, rows, 128), F32),
            pltpu.VMEM((sp // tp, rows, slice_width), BF),
            pltpu.VMEM((sp, rows, slice_width), BF),
            pltpu.VMEM((sp, tp, noted, rows), F32),
            pltpu.VMEM((sp, tp, rows // tp, columns), BF),
            pltpu.VMEM((sp, rows // tp, columns), BF),
            pltpu.VMEM((sp, rows // tp, columns), BF),
        ]
        + chunks(wide_linear)
        + chunks(wide_window)
        + [
            pltpu.VMEM((sp, sp, rows, widths[5]), BF),
            pltpu.VMEM((sp, sp, rows, widths[0]), BF),
            dma((9,)),
            dma((2,)),
            dma((sp // tp,)),
            dma((sp,)),
            dma((sp,)),
            dma,
            dma((sp * tp,)),
            dma((sp, tp)),
        ]
        + [dma((sp, sp))] * 16
        + [dma((sp,))] * 4,
        compiler_params=pltpu.CompilerParams(
            collective_id=0, has_side_effects=True, vmem_limit_bytes=56 * 2**20
        ),
    )(
        activations,
        gain,
        down,
        fade,
        decay_up_factor,
        decay_offset_bias.reshape(1, -1),
        head_sink_logit,
        linear_head_gain.reshape(1, -1),
        *matrices,
        starting_state,
    )


def mixer(*arrays):
    sp, tp = lax.axis_size("sp"), lax.axis_size("tp")
    rows = arrays[0].shape[0]
    one_each = KVH == GATED_MIXERS == sp * tp and QH % KVH == 0
    if tp == 2 and sp % tp == 0 and one_each and rows == WINDOW and rows % SPAN == 0:
        return stationary(*arrays)
    return local(*arrays)


def solution(mesh):
    placed = (
        P(("fs", "sp"), "tp"),
        P(),
        P("sp", "tp"),
        P("sp", "tp"),
        P("sp", "tp"),
        P("sp", "tp"),
        P("sp", "tp"),
        P("sp", "tp"),
        P(),
        P(None, "tp"),
        P("tp"),
        P(("fs", "sp"), "tp"),
        P("tp", None, None),
        P("tp"),
        P(),
        P("tp", "sp"),
        P("tp", "sp"),
    )
    return jax.shard_map(
        mixer, mesh=mesh, in_specs=placed, out_specs=P(("fs", "sp", "tp"), None), check_vma=False
    )
```

```python
import functools

import jax
import jax.numpy as jnp
from jax import lax
from jax.experimental import pallas as pl
from jax.experimental.pallas import tpu as pltpu
from jax.sharding import PartitionSpec as P

QH = 32
HD = 64
WINDOW = 128
LOOKUP_FEATURES = 128
DV = 256
SPAN = 64
KVH = 8
GATED_MIXERS = 8


EPS = 1e-05
FADING_SOFTNESS = 16.0
HIGH_PRECISION = lax.Precision.HIGHEST


def passed_along(value, axis, steps):
    count = lax.axis_size(axis)
    leading, last = (max(0, -steps), min(count, count - steps))
    return lax.ppermute(value, axis, [(source, source + steps) for source in range(leading, last)])


def prefix(x, axis, combine, identity):
    peers, place = (lax.axis_size(axis), lax.axis_index(axis))
    everything = jax.tree.map(
        lambda part, kind: lax.all_gather(part.astype(kind), axis), x, (jnp.bfloat16, jnp.bfloat16)
    )
    start = jax.tree.map(
        lambda part, zero: jnp.broadcast_to(jnp.asarray(zero, part.dtype), part.shape), x, identity
    )

    def hop(k, before):
        reached = k < place
        new = combine(
            before, jax.tree.map(lambda part, own: part[k].astype(own.dtype), everything, x)
        )
        return jax.tree.map(lambda a, b: jnp.where(reached, a, b), new, before)

    return lax.fori_loop(0, peers, hop, start)


def window_attention(near_query, near_keys, near_values, head_sink_logit):
    stream_extent = near_query.shape[0]
    key_heads = near_keys.shape[1] // HD
    heads_here = near_query.shape[1] // HD
    groups = heads_here // key_heads
    blocks = stream_extent // WINDOW
    tail_rows = jnp.stack([near_keys, near_values])
    before = passed_along(tail_rows, "sp", 1)

    def banded(previous, current):
        extended = jnp.concatenate([previous, current], axis=0)
        earlier = extended[:stream_extent].reshape(blocks, WINDOW, key_heads, HD)
        present = extended[WINDOW:].reshape(blocks, WINDOW, key_heads, HD)
        return jnp.concatenate([earlier, present], axis=1)

    key_band = banded(before[0], near_keys)
    value_band = banded(before[1], near_values)
    queries = near_query.reshape(blocks, WINDOW, key_heads, groups, HD)
    scores = jnp.einsum(
        "nqhgd,nkhd->hgnqk", queries, key_band, preferred_element_type=jnp.float32
    ) * HD ** (-0.5)
    head_ids = lax.axis_index("tp") * heads_here + jnp.arange(heads_here, dtype=jnp.int32)
    slopes = jnp.exp2(-8.0 * (head_ids + 1).astype(jnp.float32) / QH).reshape(key_heads, groups)
    query_pos = jnp.arange(WINDOW, dtype=jnp.int32)
    key_pos = jnp.arange(2 * WINDOW, dtype=jnp.int32)
    distance = query_pos[:, None] - key_pos[None, :] + WINDOW
    start_pos = (
        lax.axis_index("sp") * stream_extent + (jnp.arange(blocks, dtype=jnp.int32) - 1) * WINDOW
    )
    absolute = start_pos[:, None] + key_pos[None, :]
    allowed = ((distance >= 0) & (distance < WINDOW))[None] & (absolute >= 0)[:, None, :]
    biased = scores - slopes[:, :, None, None, None] * distance.astype(jnp.float32)
    weights = jnp.where(allowed, jnp.exp(biased), 0.0)
    denominator = (
        jnp.sum(weights, axis=-1, keepdims=True)
        + jnp.exp(head_sink_logit.reshape(key_heads, groups))[:, :, None, None, None]
    )
    attention = (weights / denominator).astype(jnp.bfloat16)
    attended = jnp.einsum(
        "hgnqk,nkhd->nqhgd", attention, value_band, preferred_element_type=jnp.float32
    )
    return attended.reshape(stream_extent, heads_here * HD).astype(jnp.bfloat16)


def linear_attention(
    gated_query, gated_keys, gated_values, fading_exponent, linear_head_gain, starting_state
):
    stream_extent = gated_query.shape[0]
    head_total = gated_query.shape[1] // LOOKUP_FEATURES
    span_count = stream_extent // SPAN
    scaled_query = gated_query.astype(jnp.float32).reshape(
        span_count, SPAN, head_total, LOOKUP_FEATURES
    ) * LOOKUP_FEATURES ** (-0.5)
    keys_wide = gated_keys.astype(jnp.float32).reshape(
        span_count, SPAN, head_total, LOOKUP_FEATURES
    )
    values_wide = gated_values.astype(jnp.float32).reshape(span_count, SPAN, head_total, DV)
    running = jnp.cumsum(
        fading_exponent.reshape(span_count, SPAN, head_total, LOOKUP_FEATURES), axis=1
    )
    span_end = running[:, -1]
    query_with_decay = scaled_query * jnp.exp(running)
    inverse_keys = keys_wide * jnp.exp(-running)
    ending_keys = keys_wide * jnp.exp(span_end[:, None] - running)
    inner = jnp.einsum("nchk,nshk->nhcs", query_with_decay, inverse_keys, precision=HIGH_PRECISION)
    lower = jnp.tril(jnp.ones((SPAN, SPAN), dtype=bool))
    inner = jnp.where(lower, inner, 0.0)
    within = jnp.einsum("nhcs,nshv->nchv", inner, values_wide, precision=HIGH_PRECISION)

    def advance(running_state, inputs):
        query_portion, key_portion, value_portion, scale_factor = inputs
        layer_output = jnp.einsum(
            "fmy,mys->fms", query_portion, running_state, precision=HIGH_PRECISION
        )
        running_state = running_state * scale_factor[..., None] + jnp.einsum(
            "gxp,gxz->xpz", key_portion, value_portion, precision=HIGH_PRECISION
        )
        return (running_state, layer_output)

    start_state = jnp.zeros((head_total, LOOKUP_FEATURES, DV), jnp.float32)
    state_end, carried = lax.scan(
        advance, start_state, (query_with_decay, ending_keys, values_wide, jnp.exp(span_end))
    )
    device_decay = jnp.exp(jnp.sum(span_end, axis=0))
    prefix_sums = jnp.cumsum(span_end, axis=0) - span_end

    def combine(earlier, later):
        return (earlier[0] * later[0], later[0][..., None] * earlier[1] + later[1])

    decay_before, state_before = prefix(
        (device_decay, state_end),
        "sp",
        combine,
        (jnp.ones_like(device_decay), jnp.zeros_like(state_end)),
    )
    incoming_rows = state_before + decay_before[..., None] * starting_state
    crossing = jnp.einsum(
        "qwso,soz->qwsz",
        query_with_decay * jnp.exp(prefix_sums)[:, None],
        incoming_rows,
        precision=HIGH_PRECISION,
    )
    flat = (within + carried + crossing).reshape(stream_extent, head_total, DV)
    normal = (
        flat * lax.rsqrt(jnp.mean(flat * flat, axis=-1, keepdims=True) + EPS) * linear_head_gain
    )
    return normal.reshape(stream_extent, head_total * DV).astype(jnp.bfloat16)


def local(
    activations,
    input_norm_gain,
    window_query_weight,
    window_key_weight,
    window_value_weight,
    linear_query_weight,
    linear_key_weight,
    linear_value_weight,
    decay_down_factor,
    decay_up_factor,
    decay_offset_bias,
    extra_fading_exponent,
    starting_state,
    head_sink_logit,
    linear_head_gain,
    window_output_weight,
    linear_output_weight,
):
    gathered = lax.all_gather(activations, "tp", axis=1, tiled=True)
    widened = gathered.astype(jnp.float32)
    normed = (
        widened
        * lax.rsqrt(jnp.mean(widened * widened, axis=1, keepdims=True) + EPS)
        * input_norm_gain
    ).astype(jnp.bfloat16)
    row_total = normed.shape[0]
    matrices = (
        window_query_weight,
        window_key_weight,
        window_value_weight,
        linear_query_weight,
        linear_key_weight,
        linear_value_weight,
    )
    segments = (
        lax.all_gather(matrices[0], "sp", axis=0, tiled=True),
        lax.all_gather(matrices[1], "sp", axis=0, tiled=True),
        lax.all_gather(matrices[2], "sp", axis=0, tiled=True),
        lax.all_gather(matrices[3], "sp", axis=0, tiled=True),
        lax.all_gather(matrices[4], "sp", axis=0, tiled=True),
        lax.all_gather(matrices[5], "sp", axis=0, tiled=True),
    )
    projected = tuple(
        (jnp.dot(normed, segment, preferred_element_type=jnp.float32) for segment in segments)
    )
    near_query, near_keys, near_values, gated_query, gated_keys, gated_values = [
        product.astype(jnp.bfloat16) for product in projected
    ]
    low_rank = jnp.dot(normed, decay_down_factor, preferred_element_type=jnp.float32).astype(
        jnp.bfloat16
    )
    attention_energies = (
        jnp.dot(low_rank, decay_up_factor, preferred_element_type=jnp.float32) + decay_offset_bias
    )
    head_total = extra_fading_exponent.shape[1]
    fading_exponent = (jax.nn.log_sigmoid(attention_energies) / FADING_SOFTNESS).reshape(
        row_total, head_total, LOOKUP_FEATURES
    ) + extra_fading_exponent[:, :, None]
    near_out = window_attention(near_query, near_keys, near_values, head_sink_logit)
    gated_out = linear_attention(
        gated_query, gated_keys, gated_values, fading_exponent, linear_head_gain, starting_state
    )
    window_full, linear_full = (
        lax.all_gather(window_output_weight, "sp", axis=1, tiled=True),
        lax.all_gather(linear_output_weight, "sp", axis=1, tiled=True),
    )
    return lax.psum_scatter(
        (
            jnp.dot(near_out, window_full, preferred_element_type=jnp.float32)
            + jnp.dot(gated_out, linear_full, preferred_element_type=jnp.float32)
        ).astype(jnp.bfloat16),
        "tp",
        scatter_dimension=0,
        tiled=True,
    )


MESH = pl.DeviceIdType.MESH
BF = jnp.bfloat16
F32 = jnp.float32


def dot(a, b):
    return jnp.dot(a, b, preferred_element_type=F32)


def remote(src, dst, send_sem, recv_sem, **where):
    return pltpu.make_async_remote_copy(
        src_ref=src,
        dst_ref=dst,
        send_sem=send_sem,
        recv_sem=recv_sem,
        device_id=where,
        device_id_type=MESH,
    )


def greet(sp, tp):
    s, t = lax.axis_index("sp"), lax.axis_index("tp")
    barrier = pltpu.get_barrier_semaphore()
    for ds in range(sp):
        for dt in range(tp):
            if ds or dt:
                where = {"sp": lax.rem(s + ds, sp), "tp": lax.rem(t + dt, tp)}
                pl.semaphore_signal(barrier, inc=1, device_id=where, device_id_type=MESH)
    pl.semaphore_wait(barrier, sp * tp - 1)


def columns_dot(a, b):
    return lax.dot_general(a, b, (((1,), (1,)), ((), ())), preferred_element_type=F32)


def mixer_kernel(sp, tp, widths, order, *refs):
    x, gain, down, fade, up, bias, sink, head_gain = refs[:8]
    sources, state_in, out = refs[8:16], refs[16], refs[17]
    weights, start = refs[18:26], refs[26]
    squares, normed, blocks, note, term, away, landed = refs[27:34]
    lin = refs[34:38]
    held_g, held_n = refs[38:40]
    w_sem, sq_sem, a_send, a_recv, f_send, l_sem, n_send, n_recv = refs[40:48]
    lin_sem, g_sem, h_sem = refs[48:52], refs[52:56], refs[56:60]
    t_send, t_recv, o_send, o_recv = refs[60:64]
    s, t = lax.axis_index("sp"), lax.axis_index("tp")
    other = 1 - t
    after, ahead = jnp.minimum(s + 1, sp - 1), jnp.maximum(s - 1, 0)
    per_half = sp // tp
    rows, half = x.shape
    width = half // per_half
    rank = down.shape[1]
    loads = [
        pltpu.make_async_copy(a, b, w_sem.at[i]) for i, (a, b) in enumerate(zip(sources, weights))
    ]
    loads.append(pltpu.make_async_copy(state_in.at[s], start, w_sem.at[len(sources)]))
    for i in (3, 4, 5, 0, 1, 2, 8, 6, 7):
        loads[i].start()
    wide = x[...].astype(F32)
    own = jnp.sum(wide * wide, axis=1, keepdims=True)
    squares[0] = jnp.broadcast_to(own, (rows, 128))
    greet(sp, tp)
    swap_squares = remote(squares.at[0], squares.at[1], sq_sem.at[0], sq_sem.at[1], tp=other)
    swap_squares.start()
    swap_squares.wait()
    total = own + squares[1][:, :1]
    scale = lax.rsqrt(total / (half * tp) + EPS)
    home = lax.div(s, per_half) == t

    def slice_send(i):
        j = t * per_half + i
        return remote(normed.at[i], blocks.at[s], a_send.at[i], a_recv.at[s], sp=j)

    for i in range(per_half):
        cols = slice(i * width, (i + 1) * width)
        normed[i] = (x[:, cols].astype(F32) * scale * gain[t, :, cols]).astype(BF)

        @pl.when(t * per_half + i != s)
        def _():
            slice_send(i).start()

        @pl.when(t * per_half + i == s)
        def _():
            keep = pltpu.make_async_copy(normed.at[i], blocks.at[s], l_sem)
            keep.start()
            keep.wait()

    def forward(b):
        return remote(blocks.at[b], blocks.at[b], f_send.at[b], a_recv.at[b], tp=other)

    @pl.when(home)
    def _():
        forward(s).start()

    low = jnp.zeros((rank, rows), F32)
    for i in range(per_half):
        low += columns_dot(down[t, :, i * width : (i + 1) * width], normed[i])
    note[s, t, :rank] = low
    note[s, t, rank:] = fade[...]

    def note_send(n):
        where = {"sp": lax.rem(s + n // tp, sp), "tp": lax.rem(t + n % tp, tp)}
        return remote(note.at[s, t], note.at[s, t], n_send.at[n], n_recv.at[s, t], **where)

    def right(group, sems, b, d):
        return remote(group[0].at[b, d], group[1].at[b, d], sems[0].at[b, d], sems[1].at[b, d], sp=after)

    def left(group, sems, b, d):
        return remote(group[0].at[b, d], group[2].at[b, d], sems[2].at[b, d], sems[3].at[b, d], sp=ahead)

    def ends(group, sems, b):
        @pl.when(s == 0)
        def _():
            for d in range(sp - 1, 0, -1):
                right(group, sems, b, d).start()

        @pl.when(s == sp - 1)
        def _():
            for d in range(sp - 1):
                left(group, sems, b, d).start()

    def place(k):
        return lax.rem(s + jnp.where(s < (sp + 1) // 2, k, sp - k), sp)

    for i in range(6):
        loads[i].wait()

    def project(k, carry):
        b = place(k)

        @pl.when(jnp.logical_or(jnp.logical_not(home), b != s))
        def _():
            forward(b).wait_recv()

        @pl.when(jnp.logical_and(home, b != s))
        def _():
            forward(b).start()

        block = blocks[b]
        keys = dot(block, weights[1][...])
        vals = dot(block, weights[2][...])
        kw, vw = widths[1], widths[2]
        for d in range(sp):
            at = 0
            for i in (3, 4, 5, 0):
                w = widths[i]
                lin[0][b, d, :, at : at + w] = dot(block, weights[i][:, d * w : (d + 1) * w]).astype(BF)
                at += w
            lin[0][b, d, :, at : at + kw] = keys[:, d * kw : (d + 1) * kw].astype(BF)
            lin[0][b, d, :, at + kw :] = vals[:, d * vw : (d + 1) * vw].astype(BF)
        ends(lin, lin_sem, b)
        return carry

    lax.fori_loop(0, sp, project, 0)
    for n in range(1, sp * tp):
        note_send(n).start()

    def relay(group, sems, k):
        br, bl = k, sp - 1 - k
        for n in range(sp - 1):
            dr, dl = sp - 1 - n, n

            @pl.when(jnp.logical_and(s > 0, s < dr))
            def _():
                right(group, sems, br, dr).wait_recv()
                group[0][br, dr] = (
                    group[0][br, dr].astype(F32) + group[1][br, dr].astype(F32)
                ).astype(BF)
                right(group, sems, br, dr).start()

            @pl.when(jnp.logical_and(s < sp - 1, s > dl))
            def _():
                left(group, sems, bl, dl).wait_recv()
                group[0][bl, dl] = (
                    group[0][bl, dl].astype(F32) + group[2][bl, dl].astype(F32)
                ).astype(BF)
                left(group, sems, bl, dl).start()

    def relay_step(k, carry):
        relay(lin, lin_sem, k)
        return carry

    lax.fori_loop(0, sp, relay_step, 0)

    def finish(group, sems, b):
        group[3][b] = group[0][b, s]

        @pl.when(s > 0)
        def _():
            right(group, sems, b, s).wait_recv()
            group[3][b] = (group[3][b].astype(F32) + group[1][b, s].astype(F32)).astype(BF)

        @pl.when(s < sp - 1)
        def _():
            left(group, sems, b, s).wait_recv()
            group[3][b] = (group[3][b].astype(F32) + group[2][b, s].astype(F32)).astype(BF)

    def sent(group, sems, b):
        for d in range(sp):

            @pl.when(s < d)
            def _():
                right(group, sems, b, d).wait_send()

            @pl.when(s > d)
            def _():
                left(group, sems, b, d).wait_send()

    def gather_right(held, sems, b, src):
        ref = held.at[b, src]
        return remote(ref, ref, sems[0].at[b, src], sems[1].at[b, src], sp=after)

    def gather_left(held, sems, b, src):
        ref = held.at[b, src]
        return remote(ref, ref, sems[2].at[b, src], sems[3].at[b, src], sp=ahead)

    def start_own(held, sems, b):
        @pl.when(s < sp - 1)
        def _():
            gather_right(held, sems, b, s).start()

        @pl.when(s > 0)
        def _():
            gather_left(held, sems, b, s).start()

    def pass_on(held, sems, b):
        for n in range(1, sp):

            @pl.when(s - n >= 0)
            def _():
                src = jnp.maximum(s - n, 0)
                gather_right(held, sems, b, src).wait_recv()

                @pl.when(s < sp - 1)
                def _():
                    gather_right(held, sems, b, src).start()

            @pl.when(s + n < sp)
            def _():
                src = jnp.minimum(s + n, sp - 1)
                gather_left(held, sems, b, src).wait_recv()

                @pl.when(s > 0)
                def _():
                    gather_left(held, sems, b, src).start()

    loads[8].wait()
    for n in range(1, sp * tp):
        ps, pt = lax.rem(s + n // tp, sp), lax.rem(t + n % tp, tp)
        remote(note.at[ps, pt], note.at[ps, pt], n_send.at[n], n_recv.at[ps, pt], tp=other).wait_recv()
    lk = LOOKUP_FEATURES
    lane = pl.ds(pl.multiple_of(s * lk, lk), lk)
    up_own = jnp.concatenate([up[:, lane], jnp.zeros((rows - rank, lk), BF)], axis=0)
    bias_own = bias[:, lane]
    row_at = lax.broadcasted_iota(jnp.int32, (rows, rows), 0)
    col_at = lax.broadcasted_iota(jnp.int32, (rows, rows), 1)
    span_low = jnp.logical_and(row_at >= col_at, row_at // SPAN == col_at // SPAN)
    ones_low = jnp.where(span_low, 1.0, 0.0)
    noted = note.shape[2]
    wide = sum(widths[3:])

    def linear(b, state):
        finish(lin, lin_sem, b)
        rank_rows = note[b, 0, :rank] + note[b, 1, :rank]
        tall = jnp.concatenate(
            [rank_rows, note[b, t, rank:], jnp.zeros((rows - noted, rows), F32)], axis=0
        ).T
        energies = dot(tall.astype(BF), up_own) + bias_own
        soft = jnp.minimum(energies, 0.0) - jnp.log1p(jnp.exp(-jnp.abs(energies)))
        extra = jnp.sum(jnp.where(col_at == rank + s, tall, 0.0), axis=1, keepdims=True)
        fading = soft / FADING_SOFTNESS + extra
        running = lax.dot_general(
            ones_low,
            fading,
            (((1,), (0,)), ((), ())),
            precision=HIGH_PRECISION,
            preferred_element_type=F32,
        )
        query = lin[3][b, :, :lk].astype(F32) * lk ** (-0.5)
        key = lin[3][b, :, lk : 2 * lk].astype(F32)
        value = lin[3][b, :, 2 * lk : wide]
        decayed = (query * jnp.exp(running)).astype(BF)
        inner = columns_dot(decayed, (key * jnp.exp(-running)).astype(BF))
        inner = jnp.where(span_low, inner, 0.0).astype(BF)
        within = dot(inner, value)
        carried = []
        for j in range(rows // SPAN):
            cut = slice(j * SPAN, (j + 1) * SPAN)
            end = running[(j + 1) * SPAN - 1 : (j + 1) * SPAN]
            ending = (key[cut] * jnp.exp(end - running[cut])).astype(BF)
            carried.append(columns_dot(decayed[cut], state.astype(BF)))
            state = state * jnp.exp(end) + lax.dot_general(
                value[cut], ending, (((0,), (0,)), ((), ())), preferred_element_type=F32
            )
        flat = within + jnp.concatenate(carried, axis=0)
        normal = flat * lax.rsqrt(jnp.mean(flat * flat, axis=-1, keepdims=True) + EPS) * head_gain[...]
        q, r = divmod(order.index(b), 2)
        held_g[q, s, r * rows : (r + 1) * rows] = normal.astype(BF)
        return state

    state = start[...].T
    for b in range(sp):
        state = linear(b, state)
    for q in range(sp // 2):
        start_own(held_g, g_sem, q)

    query_at = lax.broadcasted_iota(jnp.int32, (rows, 2 * rows), 0)
    key_at = lax.broadcasted_iota(jnp.int32, (rows, 2 * rows), 1)
    distance = query_at - key_at + rows
    near_by = jnp.logical_and(distance >= 0, distance < WINDOW)
    far = distance.astype(F32)
    heads = widths[0] // HD
    qw = widths[0]
    for b in order:
        present = lin[3][b, :, wide:]
        earlier = lin[3][max(b - 1, 0), :, wide:]
        keys = jnp.concatenate([earlier[:, qw : qw + HD], present[:, qw : qw + HD]], axis=0)
        vals = jnp.concatenate([earlier[:, qw + HD :], present[:, qw + HD :]], axis=0)
        allowed = near_by if b else jnp.logical_and(near_by, key_at >= rows)
        results = []
        for h in range(heads):
            number = ((t * sp + s) * heads + h + 1).astype(F32)
            slope = jnp.exp2(jnp.full((rows, 1), -8.0 / QH, F32) * number)
            score = columns_dot(present[:, h * HD : (h + 1) * HD], keys) * HD ** (-0.5) - slope * far
            weight = jnp.where(allowed, jnp.exp(score), 0.0)
            floor = jnp.exp(jnp.full((rows, 1), sink[s * heads + h], F32))
            probs = (weight / (jnp.sum(weight, axis=1, keepdims=True) + floor)).astype(BF)
            results.append(dot(probs, vals))
        q, r = divmod(order.index(b), 2)
        held_n[q, s, r * rows : (r + 1) * rows] = jnp.concatenate(results, axis=1).astype(BF)
        if r:
            start_own(held_n, h_sem, q)

    loads[6].wait()
    loads[7].wait()
    part = rows // tp
    near_cols, gated_cols = held_n.shape[3], held_g.shape[3]

    def swap(b):
        return remote(term.at[b, other], away.at[b], t_send.at[b], t_recv.at[b], tp=other)

    def deliver(b):
        return remote(term.at[b, t], landed.at[s], o_send.at[b], o_recv.at[s], sp=b)

    def close(b):
        swap(b).wait()
        term[b, t] = (term[b, t].astype(F32) + away[b].astype(F32)).astype(BF)

        @pl.when(s != b)
        def _():
            deliver(b).start()

        @pl.when(s == b)
        def _():
            landed[b] = term[b, t]

    for q in range(sp // 2):
        pass_on(held_g, g_sem, q)
    for k, b in enumerate(order):
        q, r = divmod(k, 2)
        if r == 0:
            pass_on(held_n, h_sem, q)
        if k:
            close(order[k - 1])
        total = None
        for src in range(sp):
            piece = dot(held_n[q, src, r * rows : (r + 1) * rows], weights[6][src * near_cols : (src + 1) * near_cols]) + dot(
                held_g[q, src, r * rows : (r + 1) * rows], weights[7][src * gated_cols : (src + 1) * gated_cols]
            )
            total = piece if total is None else total + piece
        for h in range(tp):
            term[b, h] = total[h * part : (h + 1) * part].astype(BF)
        swap(b).start()
    close(order[-1])

    def drain(b, carry):
        sent(lin, lin_sem, b)

        @pl.when(home)
        def _():
            forward(b).wait_send()

        return carry

    lax.fori_loop(0, sp, drain, 0)
    for held, sems in ((held_g, g_sem), (held_n, h_sem)):
        for q in range(sp // 2):
            for src in range(sp):

                @pl.when(jnp.logical_and(src <= s, s < sp - 1))
                def _():
                    gather_right(held, sems, q, src).wait_send()

                @pl.when(jnp.logical_and(src >= s, s > 0))
                def _():
                    gather_left(held, sems, q, src).wait_send()

    for i in range(per_half):

        @pl.when(t * per_half + i != s)
        def _():
            slice_send(i).wait_send()

    for n in range(1, sp * tp):
        note_send(n).wait_send()
    columns = landed.shape[2]
    for b in range(sp):

        @pl.when(s != b)
        def _():
            deliver(b).wait_send()
            remote(landed.at[b], landed.at[b], o_send.at[b], o_recv.at[b], tp=other).wait_recv()

        out[:, b * columns : (b + 1) * columns] = landed[b]


def stationary(
    activations,
    input_norm_gain,
    window_query_weight,
    window_key_weight,
    window_value_weight,
    linear_query_weight,
    linear_key_weight,
    linear_value_weight,
    decay_down_factor,
    decay_up_factor,
    decay_offset_bias,
    extra_fading_exponent,
    starting_state,
    head_sink_logit,
    linear_head_gain,
    window_output_weight,
    linear_output_weight,
):
    sp, tp = lax.axis_size("sp"), lax.axis_size("tp")
    rows, half = activations.shape
    matrices = (
        window_query_weight,
        window_key_weight,
        window_value_weight,
        linear_query_weight,
        linear_key_weight,
        linear_value_weight,
        window_output_weight,
        linear_output_weight,
    )
    widths = tuple(m.shape[1] // sp for m in matrices[:6])
    rank = decay_down_factor.shape[1]
    heads_tp = extra_fading_exponent.shape[1]
    gain = input_norm_gain.reshape(tp, 1, half)
    down = decay_down_factor.T.reshape(rank, tp, half).transpose(1, 0, 2)
    fade = jnp.pad(extra_fading_exponent.T, ((0, -heads_tp % 8), (0, 0)))
    noted = rank + fade.shape[0]
    columns = window_output_weight.shape[1]
    order = sorted(range(sp), key=lambda b: -abs(2 * b - sp + 1))
    vmem = pl.BlockSpec(memory_space=pltpu.VMEM)
    hbm = pl.BlockSpec(memory_space=pltpu.HBM)
    dma = pltpu.SemaphoreType.DMA
    slice_width = half * tp // sp

    def chunks(cols):
        return [pltpu.VMEM((sp, sp, rows, cols), BF)] * 3 + [pltpu.VMEM((sp, rows, cols), BF)]

    return pl.pallas_call(
        functools.partial(mixer_kernel, sp, tp, widths, order),
        out_shape=jax.ShapeDtypeStruct((rows // tp, columns * sp), BF),
        in_specs=[vmem] * 6
        + [pl.BlockSpec(memory_space=pltpu.SMEM), vmem]
        + [hbm] * 9,
        out_specs=vmem,
        scratch_shapes=[pltpu.VMEM(m.shape, BF) for m in matrices]
        + [
            pltpu.VMEM(starting_state.shape[1:], F32),
            pltpu.VMEM((2, rows, 128), F32),
            pltpu.VMEM((sp // tp, rows, slice_width), BF),
            pltpu.VMEM((sp, rows, slice_width), BF),
            pltpu.VMEM((sp, tp, noted, rows), F32),
            pltpu.VMEM((sp, tp, rows // tp, columns), BF),
            pltpu.VMEM((sp, rows // tp, columns), BF),
            pltpu.VMEM((sp, rows // tp, columns), BF),
        ]
        + chunks(sum(widths))
        + [
            pltpu.VMEM((sp // 2, sp, 2 * rows, widths[5]), BF),
            pltpu.VMEM((sp // 2, sp, 2 * rows, widths[0]), BF),
            dma((9,)),
            dma((2,)),
            dma((sp // tp,)),
            dma((sp,)),
            dma((sp,)),
            dma,
            dma((sp * tp,)),
            dma((sp, tp)),
        ]
        + [dma((sp, sp))] * 12
        + [dma((sp,))] * 4,
        compiler_params=pltpu.CompilerParams(
            collective_id=0, has_side_effects=True, vmem_limit_bytes=56 * 2**20
        ),
    )(
        activations,
        gain,
        down,
        fade,
        decay_up_factor,
        decay_offset_bias.reshape(1, -1),
        head_sink_logit,
        linear_head_gain.reshape(1, -1),
        *matrices,
        starting_state,
    )


def mixer(*arrays):
    sp, tp = lax.axis_size("sp"), lax.axis_size("tp")
    rows = arrays[0].shape[0]
    one_each = KVH == GATED_MIXERS == sp * tp and QH % KVH == 0
    if tp == 2 and sp % tp == 0 and one_each and rows == WINDOW and rows % SPAN == 0:
        return stationary(*arrays)
    return local(*arrays)


def solution(mesh):
    placed = (
        P(("fs", "sp"), "tp"),
        P(),
        P("sp", "tp"),
        P("sp", "tp"),
        P("sp", "tp"),
        P("sp", "tp"),
        P("sp", "tp"),
        P("sp", "tp"),
        P(),
        P(None, "tp"),
        P("tp"),
        P(("fs", "sp"), "tp"),
        P("tp", None, None),
        P("tp"),
        P(),
        P("tp", "sp"),
        P("tp", "sp"),
    )
    return jax.shard_map(
        mixer, mesh=mesh, in_specs=placed, out_specs=P(("fs", "sp", "tp"), None), check_vma=False
    )
```

```python
import functools

import jax
import jax.numpy as jnp
from jax import lax
from jax.experimental import pallas as pl
from jax.experimental.pallas import tpu as pltpu
from jax.sharding import PartitionSpec as P

QH = 32
HD = 64
WINDOW = 128
LOOKUP_FEATURES = 128
DV = 256
SPAN = 64
KVH = 8
GATED_MIXERS = 8


EPS = 1e-05
FADING_SOFTNESS = 16.0
HIGH_PRECISION = lax.Precision.HIGHEST


def passed_along(value, axis, steps):
    count = lax.axis_size(axis)
    leading, last = (max(0, -steps), min(count, count - steps))
    return lax.ppermute(value, axis, [(source, source + steps) for source in range(leading, last)])


def prefix(x, axis, combine, identity):
    peers, place = (lax.axis_size(axis), lax.axis_index(axis))
    everything = jax.tree.map(
        lambda part, kind: lax.all_gather(part.astype(kind), axis), x, (jnp.bfloat16, jnp.bfloat16)
    )
    start = jax.tree.map(
        lambda part, zero: jnp.broadcast_to(jnp.asarray(zero, part.dtype), part.shape), x, identity
    )

    def hop(k, before):
        reached = k < place
        new = combine(
            before, jax.tree.map(lambda part, own: part[k].astype(own.dtype), everything, x)
        )
        return jax.tree.map(lambda a, b: jnp.where(reached, a, b), new, before)

    return lax.fori_loop(0, peers, hop, start)


def window_attention(near_query, near_keys, near_values, head_sink_logit):
    stream_extent = near_query.shape[0]
    key_heads = near_keys.shape[1] // HD
    heads_here = near_query.shape[1] // HD
    groups = heads_here // key_heads
    blocks = stream_extent // WINDOW
    tail_rows = jnp.stack([near_keys, near_values])
    before = passed_along(tail_rows, "sp", 1)

    def banded(previous, current):
        extended = jnp.concatenate([previous, current], axis=0)
        earlier = extended[:stream_extent].reshape(blocks, WINDOW, key_heads, HD)
        present = extended[WINDOW:].reshape(blocks, WINDOW, key_heads, HD)
        return jnp.concatenate([earlier, present], axis=1)

    key_band = banded(before[0], near_keys)
    value_band = banded(before[1], near_values)
    queries = near_query.reshape(blocks, WINDOW, key_heads, groups, HD)
    scores = jnp.einsum(
        "nqhgd,nkhd->hgnqk", queries, key_band, preferred_element_type=jnp.float32
    ) * HD ** (-0.5)
    head_ids = lax.axis_index("tp") * heads_here + jnp.arange(heads_here, dtype=jnp.int32)
    slopes = jnp.exp2(-8.0 * (head_ids + 1).astype(jnp.float32) / QH).reshape(key_heads, groups)
    query_pos = jnp.arange(WINDOW, dtype=jnp.int32)
    key_pos = jnp.arange(2 * WINDOW, dtype=jnp.int32)
    distance = query_pos[:, None] - key_pos[None, :] + WINDOW
    start_pos = (
        lax.axis_index("sp") * stream_extent + (jnp.arange(blocks, dtype=jnp.int32) - 1) * WINDOW
    )
    absolute = start_pos[:, None] + key_pos[None, :]
    allowed = ((distance >= 0) & (distance < WINDOW))[None] & (absolute >= 0)[:, None, :]
    biased = scores - slopes[:, :, None, None, None] * distance.astype(jnp.float32)
    weights = jnp.where(allowed, jnp.exp(biased), 0.0)
    denominator = (
        jnp.sum(weights, axis=-1, keepdims=True)
        + jnp.exp(head_sink_logit.reshape(key_heads, groups))[:, :, None, None, None]
    )
    attention = (weights / denominator).astype(jnp.bfloat16)
    attended = jnp.einsum(
        "hgnqk,nkhd->nqhgd", attention, value_band, preferred_element_type=jnp.float32
    )
    return attended.reshape(stream_extent, heads_here * HD).astype(jnp.bfloat16)


def linear_attention(
    gated_query, gated_keys, gated_values, fading_exponent, linear_head_gain, starting_state
):
    stream_extent = gated_query.shape[0]
    head_total = gated_query.shape[1] // LOOKUP_FEATURES
    span_count = stream_extent // SPAN
    scaled_query = gated_query.astype(jnp.float32).reshape(
        span_count, SPAN, head_total, LOOKUP_FEATURES
    ) * LOOKUP_FEATURES ** (-0.5)
    keys_wide = gated_keys.astype(jnp.float32).reshape(
        span_count, SPAN, head_total, LOOKUP_FEATURES
    )
    values_wide = gated_values.astype(jnp.float32).reshape(span_count, SPAN, head_total, DV)
    running = jnp.cumsum(
        fading_exponent.reshape(span_count, SPAN, head_total, LOOKUP_FEATURES), axis=1
    )
    span_end = running[:, -1]
    query_with_decay = scaled_query * jnp.exp(running)
    inverse_keys = keys_wide * jnp.exp(-running)
    ending_keys = keys_wide * jnp.exp(span_end[:, None] - running)
    inner = jnp.einsum("nchk,nshk->nhcs", query_with_decay, inverse_keys, precision=HIGH_PRECISION)
    lower = jnp.tril(jnp.ones((SPAN, SPAN), dtype=bool))
    inner = jnp.where(lower, inner, 0.0)
    within = jnp.einsum("nhcs,nshv->nchv", inner, values_wide, precision=HIGH_PRECISION)

    def advance(running_state, inputs):
        query_portion, key_portion, value_portion, scale_factor = inputs
        layer_output = jnp.einsum(
            "fmy,mys->fms", query_portion, running_state, precision=HIGH_PRECISION
        )
        running_state = running_state * scale_factor[..., None] + jnp.einsum(
            "gxp,gxz->xpz", key_portion, value_portion, precision=HIGH_PRECISION
        )
        return (running_state, layer_output)

    start_state = jnp.zeros((head_total, LOOKUP_FEATURES, DV), jnp.float32)
    state_end, carried = lax.scan(
        advance, start_state, (query_with_decay, ending_keys, values_wide, jnp.exp(span_end))
    )
    device_decay = jnp.exp(jnp.sum(span_end, axis=0))
    prefix_sums = jnp.cumsum(span_end, axis=0) - span_end

    def combine(earlier, later):
        return (earlier[0] * later[0], later[0][..., None] * earlier[1] + later[1])

    decay_before, state_before = prefix(
        (device_decay, state_end),
        "sp",
        combine,
        (jnp.ones_like(device_decay), jnp.zeros_like(state_end)),
    )
    incoming_rows = state_before + decay_before[..., None] * starting_state
    crossing = jnp.einsum(
        "qwso,soz->qwsz",
        query_with_decay * jnp.exp(prefix_sums)[:, None],
        incoming_rows,
        precision=HIGH_PRECISION,
    )
    flat = (within + carried + crossing).reshape(stream_extent, head_total, DV)
    normal = (
        flat * lax.rsqrt(jnp.mean(flat * flat, axis=-1, keepdims=True) + EPS) * linear_head_gain
    )
    return normal.reshape(stream_extent, head_total * DV).astype(jnp.bfloat16)


def local(
    activations,
    input_norm_gain,
    window_query_weight,
    window_key_weight,
    window_value_weight,
    linear_query_weight,
    linear_key_weight,
    linear_value_weight,
    decay_down_factor,
    decay_up_factor,
    decay_offset_bias,
    extra_fading_exponent,
    starting_state,
    head_sink_logit,
    linear_head_gain,
    window_output_weight,
    linear_output_weight,
):
    gathered = lax.all_gather(activations, "tp", axis=1, tiled=True)
    widened = gathered.astype(jnp.float32)
    normed = (
        widened
        * lax.rsqrt(jnp.mean(widened * widened, axis=1, keepdims=True) + EPS)
        * input_norm_gain
    ).astype(jnp.bfloat16)
    row_total = normed.shape[0]
    matrices = (
        window_query_weight,
        window_key_weight,
        window_value_weight,
        linear_query_weight,
        linear_key_weight,
        linear_value_weight,
    )
    segments = (
        lax.all_gather(matrices[0], "sp", axis=0, tiled=True),
        lax.all_gather(matrices[1], "sp", axis=0, tiled=True),
        lax.all_gather(matrices[2], "sp", axis=0, tiled=True),
        lax.all_gather(matrices[3], "sp", axis=0, tiled=True),
        lax.all_gather(matrices[4], "sp", axis=0, tiled=True),
        lax.all_gather(matrices[5], "sp", axis=0, tiled=True),
    )
    projected = tuple(
        (jnp.dot(normed, segment, preferred_element_type=jnp.float32) for segment in segments)
    )
    near_query, near_keys, near_values, gated_query, gated_keys, gated_values = [
        product.astype(jnp.bfloat16) for product in projected
    ]
    low_rank = jnp.dot(normed, decay_down_factor, preferred_element_type=jnp.float32).astype(
        jnp.bfloat16
    )
    attention_energies = (
        jnp.dot(low_rank, decay_up_factor, preferred_element_type=jnp.float32) + decay_offset_bias
    )
    head_total = extra_fading_exponent.shape[1]
    fading_exponent = (jax.nn.log_sigmoid(attention_energies) / FADING_SOFTNESS).reshape(
        row_total, head_total, LOOKUP_FEATURES
    ) + extra_fading_exponent[:, :, None]
    near_out = window_attention(near_query, near_keys, near_values, head_sink_logit)
    gated_out = linear_attention(
        gated_query, gated_keys, gated_values, fading_exponent, linear_head_gain, starting_state
    )
    window_full, linear_full = (
        lax.all_gather(window_output_weight, "sp", axis=1, tiled=True),
        lax.all_gather(linear_output_weight, "sp", axis=1, tiled=True),
    )
    return lax.psum_scatter(
        (
            jnp.dot(near_out, window_full, preferred_element_type=jnp.float32)
            + jnp.dot(gated_out, linear_full, preferred_element_type=jnp.float32)
        ).astype(jnp.bfloat16),
        "tp",
        scatter_dimension=0,
        tiled=True,
    )


MESH = pl.DeviceIdType.MESH
BF = jnp.bfloat16
F32 = jnp.float32


def dot(a, b):
    return jnp.dot(a, b, preferred_element_type=F32)


def remote(src, dst, send_sem, recv_sem, **where):
    return pltpu.make_async_remote_copy(
        src_ref=src,
        dst_ref=dst,
        send_sem=send_sem,
        recv_sem=recv_sem,
        device_id=where,
        device_id_type=MESH,
    )


def greet(sp, tp):
    s, t = lax.axis_index("sp"), lax.axis_index("tp")
    barrier = pltpu.get_barrier_semaphore()
    for ds in range(sp):
        for dt in range(tp):
            if ds or dt:
                where = {"sp": lax.rem(s + ds, sp), "tp": lax.rem(t + dt, tp)}
                pl.semaphore_signal(barrier, inc=1, device_id=where, device_id_type=MESH)
    pl.semaphore_wait(barrier, sp * tp - 1)


def columns_dot(a, b):
    return lax.dot_general(a, b, (((1,), (1,)), ((), ())), preferred_element_type=F32)


def mixer_kernel(sp, tp, widths, order, *refs):
    x, gain, down, fade, up, bias, sink, head_gain = refs[:8]
    sources, state_in, out = refs[8:16], refs[16], refs[17]
    weights, start = refs[18:26], refs[26]
    squares, normed, blocks, note, term, away, landed = refs[27:34]
    lin = refs[34:38]
    held_g, held_n = refs[38:40]
    w_sem, sq_sem, a_send, a_recv, f_send, l_sem, n_send, n_recv = refs[40:48]
    lin_sem, g_sem, h_sem = refs[48:52], refs[52:56], refs[56:60]
    t_send, t_recv, o_send, o_recv = refs[60:64]
    s, t = lax.axis_index("sp"), lax.axis_index("tp")
    other = 1 - t
    after, ahead = jnp.minimum(s + 1, sp - 1), jnp.maximum(s - 1, 0)
    per_half = sp // tp
    rows, half = x.shape
    width = half // per_half
    rank = down.shape[1]
    loads = [
        pltpu.make_async_copy(a, b, w_sem.at[i]) for i, (a, b) in enumerate(zip(sources, weights))
    ]
    loads.append(pltpu.make_async_copy(state_in.at[s], start, w_sem.at[len(sources)]))
    for i in (3, 4, 5, 0, 1, 2, 8, 6, 7):
        loads[i].start()
    wide = x[...].astype(F32)
    own = jnp.sum(wide * wide, axis=1, keepdims=True)
    squares[0] = jnp.broadcast_to(own, (rows, 128))
    greet(sp, tp)
    swap_squares = remote(squares.at[0], squares.at[1], sq_sem.at[0], sq_sem.at[1], tp=other)
    swap_squares.start()
    swap_squares.wait()
    total = own + squares[1][:, :1]
    scale = lax.rsqrt(total / (half * tp) + EPS)
    home = lax.div(s, per_half) == t

    def slice_send(i):
        j = t * per_half + i
        return remote(normed.at[i], blocks.at[s], a_send.at[i], a_recv.at[s], sp=j)

    for i in range(per_half):
        cols = slice(i * width, (i + 1) * width)
        normed[i] = (x[:, cols].astype(F32) * scale * gain[t, :, cols]).astype(BF)

        @pl.when(t * per_half + i != s)
        def _():
            slice_send(i).start()

        @pl.when(t * per_half + i == s)
        def _():
            keep = pltpu.make_async_copy(normed.at[i], blocks.at[s], l_sem)
            keep.start()
            keep.wait()

    def forward(b):
        return remote(blocks.at[b], blocks.at[b], f_send.at[b], a_recv.at[b], tp=other)

    @pl.when(home)
    def _():
        forward(s).start()

    low = jnp.zeros((rank, rows), F32)
    for i in range(per_half):
        low += columns_dot(down[t, :, i * width : (i + 1) * width], normed[i])
    note[s, t, :rank] = low
    note[s, t, rank:] = fade[...]

    def note_send(n):
        where = {"sp": lax.rem(s + n // tp, sp), "tp": lax.rem(t + n % tp, tp)}
        return remote(note.at[s, t], note.at[s, t], n_send.at[n], n_recv.at[s, t], **where)

    def right(group, sems, b, d):
        return remote(group[0].at[b, d], group[1].at[b, d], sems[0].at[b, d], sems[1].at[b, d], sp=after)

    def left(group, sems, b, d):
        return remote(group[0].at[b, d], group[2].at[b, d], sems[2].at[b, d], sems[3].at[b, d], sp=ahead)

    def ends(group, sems, k):
        for n in range(2):

            @pl.when(jnp.logical_and(s == 0, k == 0))
            def _():
                right(group, sems, 0, sp - 1 - n).start()

            @pl.when(jnp.logical_and(s == sp - 1, k == 0))
            def _():
                left(group, sems, sp - 1, n).start()

    def paced(group, sems, k, n):
        ready = k >= 0 if n > 1 else k >= 1
        k_old, n_old = (k, n - 2) if n > 1 else (k - 1, n + sp - 3)

        @pl.when(jnp.logical_and(s == 0, ready))
        def _():
            right(group, sems, k_old, sp - 1 - n_old).wait_send()
            right(group, sems, k, sp - 1 - n).start()

        @pl.when(jnp.logical_and(s == sp - 1, ready))
        def _():
            left(group, sems, sp - 1 - k_old, n_old).wait_send()
            left(group, sems, sp - 1 - k, n).start()

    def place(k):
        return lax.rem(s + jnp.where(s < (sp + 1) // 2, k, sp - k), sp)

    for i in range(6):
        loads[i].wait()

    def project(k, carry):
        b = place(k)

        @pl.when(jnp.logical_or(jnp.logical_not(home), b != s))
        def _():
            forward(b).wait_recv()

        @pl.when(jnp.logical_and(home, b != s))
        def _():
            forward(b).start()

        block = blocks[b]
        keys = dot(block, weights[1][...])
        vals = dot(block, weights[2][...])
        kw, vw = widths[1], widths[2]
        for d in range(sp):
            at = 0
            for i in (3, 4, 5, 0):
                w = widths[i]
                lin[0][b, d, :, at : at + w] = dot(block, weights[i][:, d * w : (d + 1) * w]).astype(BF)
                at += w
            lin[0][b, d, :, at : at + kw] = keys[:, d * kw : (d + 1) * kw].astype(BF)
            lin[0][b, d, :, at + kw :] = vals[:, d * vw : (d + 1) * vw].astype(BF)
        ends(lin, lin_sem, k)
        return carry

    lax.fori_loop(0, sp, project, 0)
    for n in range(1, sp * tp):
        note_send(n).start()

    def relay(group, sems, k):
        br, bl = k, sp - 1 - k
        for n in range(sp - 1):
            dr, dl = sp - 1 - n, n
            paced(group, sems, k, n)

            @pl.when(jnp.logical_and(s > 0, s < dr))
            def _():
                right(group, sems, br, dr).wait_recv()
                group[0][br, dr] = (
                    group[0][br, dr].astype(F32) + group[1][br, dr].astype(F32)
                ).astype(BF)
                right(group, sems, br, dr).start()

            @pl.when(jnp.logical_and(s < sp - 1, s > dl))
            def _():
                left(group, sems, bl, dl).wait_recv()
                group[0][bl, dl] = (
                    group[0][bl, dl].astype(F32) + group[2][bl, dl].astype(F32)
                ).astype(BF)
                left(group, sems, bl, dl).start()

    def relay_step(k, carry):
        relay(lin, lin_sem, k)
        return carry

    lax.fori_loop(0, sp, relay_step, 0)

    def finish(group, sems, b):
        group[3][b] = group[0][b, s]

        @pl.when(s > 0)
        def _():
            right(group, sems, b, s).wait_recv()
            group[3][b] = (group[3][b].astype(F32) + group[1][b, s].astype(F32)).astype(BF)

        @pl.when(s < sp - 1)
        def _():
            left(group, sems, b, s).wait_recv()
            group[3][b] = (group[3][b].astype(F32) + group[2][b, s].astype(F32)).astype(BF)

    def sent(group, sems, b):
        for d in range(sp):
            last_right = jnp.logical_or(s > 0, jnp.logical_and(b == sp - 1, d <= 2))
            last_left = jnp.logical_or(s < sp - 1, jnp.logical_and(b == 0, d >= sp - 3))

            @pl.when(jnp.logical_and(s < d, last_right))
            def _():
                right(group, sems, b, d).wait_send()

            @pl.when(jnp.logical_and(s > d, last_left))
            def _():
                left(group, sems, b, d).wait_send()

    def gather_right(held, sems, b, src):
        ref = held.at[b, src]
        return remote(ref, ref, sems[0].at[b, src], sems[1].at[b, src], sp=after)

    def gather_left(held, sems, b, src):
        ref = held.at[b, src]
        return remote(ref, ref, sems[2].at[b, src], sems[3].at[b, src], sp=ahead)

    def start_own(held, sems, b):
        @pl.when(s < sp - 1)
        def _():
            gather_right(held, sems, b, s).start()

        @pl.when(s > 0)
        def _():
            gather_left(held, sems, b, s).start()

    def pass_on(held, sems, b):
        for n in range(1, sp):

            @pl.when(s - n >= 0)
            def _():
                src = jnp.maximum(s - n, 0)
                gather_right(held, sems, b, src).wait_recv()

                @pl.when(s < sp - 1)
                def _():
                    gather_right(held, sems, b, src).start()

            @pl.when(s + n < sp)
            def _():
                src = jnp.minimum(s + n, sp - 1)
                gather_left(held, sems, b, src).wait_recv()

                @pl.when(s > 0)
                def _():
                    gather_left(held, sems, b, src).start()

    loads[8].wait()
    for n in range(1, sp * tp):
        ps, pt = lax.rem(s + n // tp, sp), lax.rem(t + n % tp, tp)
        remote(note.at[ps, pt], note.at[ps, pt], n_send.at[n], n_recv.at[ps, pt], tp=other).wait_recv()
    lk = LOOKUP_FEATURES
    lane = pl.ds(pl.multiple_of(s * lk, lk), lk)
    up_own = jnp.concatenate([up[:, lane], jnp.zeros((rows - rank, lk), BF)], axis=0)
    bias_own = bias[:, lane]
    row_at = lax.broadcasted_iota(jnp.int32, (rows, rows), 0)
    col_at = lax.broadcasted_iota(jnp.int32, (rows, rows), 1)
    span_low = jnp.logical_and(row_at >= col_at, row_at // SPAN == col_at // SPAN)
    ones_low = jnp.where(span_low, 1.0, 0.0)
    noted = note.shape[2]
    wide = sum(widths[3:])

    def linear(b, state):
        finish(lin, lin_sem, b)
        rank_rows = note[b, 0, :rank] + note[b, 1, :rank]
        tall = jnp.concatenate(
            [rank_rows, note[b, t, rank:], jnp.zeros((rows - noted, rows), F32)], axis=0
        ).T
        energies = dot(tall.astype(BF), up_own) + bias_own
        soft = jnp.minimum(energies, 0.0) - jnp.log1p(jnp.exp(-jnp.abs(energies)))
        extra = jnp.sum(jnp.where(col_at == rank + s, tall, 0.0), axis=1, keepdims=True)
        fading = soft / FADING_SOFTNESS + extra
        running = lax.dot_general(
            ones_low,
            fading,
            (((1,), (0,)), ((), ())),
            precision=HIGH_PRECISION,
            preferred_element_type=F32,
        )
        query = lin[3][b, :, :lk].astype(F32) * lk ** (-0.5)
        key = lin[3][b, :, lk : 2 * lk].astype(F32)
        value = lin[3][b, :, 2 * lk : wide]
        decayed = (query * jnp.exp(running)).astype(BF)
        inner = columns_dot(decayed, (key * jnp.exp(-running)).astype(BF))
        inner = jnp.where(span_low, inner, 0.0).astype(BF)
        within = dot(inner, value)
        carried = []
        for j in range(rows // SPAN):
            cut = slice(j * SPAN, (j + 1) * SPAN)
            end = running[(j + 1) * SPAN - 1 : (j + 1) * SPAN]
            ending = (key[cut] * jnp.exp(end - running[cut])).astype(BF)
            carried.append(columns_dot(decayed[cut], state.astype(BF)))
            state = state * jnp.exp(end) + lax.dot_general(
                value[cut], ending, (((0,), (0,)), ((), ())), preferred_element_type=F32
            )
        flat = within + jnp.concatenate(carried, axis=0)
        normal = flat * lax.rsqrt(jnp.mean(flat * flat, axis=-1, keepdims=True) + EPS) * head_gain[...]
        q, r = divmod(order.index(b), 2)
        held_g[q, s, r * rows : (r + 1) * rows] = normal.astype(BF)
        return state

    state = start[...].T
    for b in range(sp):
        state = linear(b, state)
    for q in range(sp // 2):
        start_own(held_g, g_sem, q)

    query_at = lax.broadcasted_iota(jnp.int32, (rows, 2 * rows), 0)
    key_at = lax.broadcasted_iota(jnp.int32, (rows, 2 * rows), 1)
    distance = query_at - key_at + rows
    near_by = jnp.logical_and(distance >= 0, distance < WINDOW)
    far = distance.astype(F32)
    heads = widths[0] // HD
    qw = widths[0]
    for b in order:
        present = lin[3][b, :, wide:]
        earlier = lin[3][max(b - 1, 0), :, wide:]
        keys = jnp.concatenate([earlier[:, qw : qw + HD], present[:, qw : qw + HD]], axis=0)
        vals = jnp.concatenate([earlier[:, qw + HD :], present[:, qw + HD :]], axis=0)
        allowed = near_by if b else jnp.logical_and(near_by, key_at >= rows)
        results = []
        for h in range(heads):
            number = ((t * sp + s) * heads + h + 1).astype(F32)
            slope = jnp.exp2(jnp.full((rows, 1), -8.0 / QH, F32) * number)
            score = columns_dot(present[:, h * HD : (h + 1) * HD], keys) * HD ** (-0.5) - slope * far
            weight = jnp.where(allowed, jnp.exp(score), 0.0)
            floor = jnp.exp(jnp.full((rows, 1), sink[s * heads + h], F32))
            probs = (weight / (jnp.sum(weight, axis=1, keepdims=True) + floor)).astype(BF)
            results.append(dot(probs, vals))
        q, r = divmod(order.index(b), 2)
        held_n[q, s, r * rows : (r + 1) * rows] = jnp.concatenate(results, axis=1).astype(BF)
        if r:
            start_own(held_n, h_sem, q)

    loads[6].wait()
    loads[7].wait()
    part = rows // tp
    near_cols, gated_cols = held_n.shape[3], held_g.shape[3]

    def swap(b):
        return remote(term.at[b, other], away.at[b], t_send.at[b], t_recv.at[b], tp=other)

    def deliver(b):
        return remote(term.at[b, t], landed.at[s], o_send.at[b], o_recv.at[s], sp=b)

    def close(b):
        swap(b).wait()
        term[b, t] = (term[b, t].astype(F32) + away[b].astype(F32)).astype(BF)

        @pl.when(s != b)
        def _():
            deliver(b).start()

        @pl.when(s == b)
        def _():
            landed[b] = term[b, t]

    for q in range(sp // 2):
        pass_on(held_g, g_sem, q)
    for k, b in enumerate(order):
        q, r = divmod(k, 2)
        if r == 0:
            pass_on(held_n, h_sem, q)
        if k:
            close(order[k - 1])
        total = None
        for src in range(sp):
            piece = dot(held_n[q, src, r * rows : (r + 1) * rows], weights[6][src * near_cols : (src + 1) * near_cols]) + dot(
                held_g[q, src, r * rows : (r + 1) * rows], weights[7][src * gated_cols : (src + 1) * gated_cols]
            )
            total = piece if total is None else total + piece
        for h in range(tp):
            term[b, h] = total[h * part : (h + 1) * part].astype(BF)
        swap(b).start()
    close(order[-1])

    def drain(b, carry):
        sent(lin, lin_sem, b)

        @pl.when(home)
        def _():
            forward(b).wait_send()

        return carry

    lax.fori_loop(0, sp, drain, 0)
    for held, sems in ((held_g, g_sem), (held_n, h_sem)):
        for q in range(sp // 2):
            for src in range(sp):

                @pl.when(jnp.logical_and(src <= s, s < sp - 1))
                def _():
                    gather_right(held, sems, q, src).wait_send()

                @pl.when(jnp.logical_and(src >= s, s > 0))
                def _():
                    gather_left(held, sems, q, src).wait_send()

    for i in range(per_half):

        @pl.when(t * per_half + i != s)
        def _():
            slice_send(i).wait_send()

    for n in range(1, sp * tp):
        note_send(n).wait_send()
    columns = landed.shape[2]
    for b in range(sp):

        @pl.when(s != b)
        def _():
            deliver(b).wait_send()
            remote(landed.at[b], landed.at[b], o_send.at[b], o_recv.at[b], tp=other).wait_recv()

        out[:, b * columns : (b + 1) * columns] = landed[b]


def stationary(
    activations,
    input_norm_gain,
    window_query_weight,
    window_key_weight,
    window_value_weight,
    linear_query_weight,
    linear_key_weight,
    linear_value_weight,
    decay_down_factor,
    decay_up_factor,
    decay_offset_bias,
    extra_fading_exponent,
    starting_state,
    head_sink_logit,
    linear_head_gain,
    window_output_weight,
    linear_output_weight,
):
    sp, tp = lax.axis_size("sp"), lax.axis_size("tp")
    rows, half = activations.shape
    matrices = (
        window_query_weight,
        window_key_weight,
        window_value_weight,
        linear_query_weight,
        linear_key_weight,
        linear_value_weight,
        window_output_weight,
        linear_output_weight,
    )
    widths = tuple(m.shape[1] // sp for m in matrices[:6])
    rank = decay_down_factor.shape[1]
    heads_tp = extra_fading_exponent.shape[1]
    gain = input_norm_gain.reshape(tp, 1, half)
    down = decay_down_factor.T.reshape(rank, tp, half).transpose(1, 0, 2)
    fade = jnp.pad(extra_fading_exponent.T, ((0, -heads_tp % 8), (0, 0)))
    noted = rank + fade.shape[0]
    columns = window_output_weight.shape[1]
    order = sorted(range(sp), key=lambda b: -abs(2 * b - sp + 1))
    vmem = pl.BlockSpec(memory_space=pltpu.VMEM)
    hbm = pl.BlockSpec(memory_space=pltpu.HBM)
    dma = pltpu.SemaphoreType.DMA
    slice_width = half * tp // sp

    def chunks(cols):
        return [pltpu.VMEM((sp, sp, rows, cols), BF)] * 3 + [pltpu.VMEM((sp, rows, cols), BF)]

    return pl.pallas_call(
        functools.partial(mixer_kernel, sp, tp, widths, order),
        out_shape=jax.ShapeDtypeStruct((rows // tp, columns * sp), BF),
        in_specs=[vmem] * 6
        + [pl.BlockSpec(memory_space=pltpu.SMEM), vmem]
        + [hbm] * 9,
        out_specs=vmem,
        scratch_shapes=[pltpu.VMEM(m.shape, BF) for m in matrices]
        + [
            pltpu.VMEM(starting_state.shape[1:], F32),
            pltpu.VMEM((2, rows, 128), F32),
            pltpu.VMEM((sp // tp, rows, slice_width), BF),
            pltpu.VMEM((sp, rows, slice_width), BF),
            pltpu.VMEM((sp, tp, noted, rows), F32),
            pltpu.VMEM((sp, tp, rows // tp, columns), BF),
            pltpu.VMEM((sp, rows // tp, columns), BF),
            pltpu.VMEM((sp, rows // tp, columns), BF),
        ]
        + chunks(sum(widths))
        + [
            pltpu.VMEM((sp // 2, sp, 2 * rows, widths[5]), BF),
            pltpu.VMEM((sp // 2, sp, 2 * rows, widths[0]), BF),
            dma((9,)),
            dma((2,)),
            dma((sp // tp,)),
            dma((sp,)),
            dma((sp,)),
            dma,
            dma((sp * tp,)),
            dma((sp, tp)),
        ]
        + [dma((sp, sp))] * 12
        + [dma((sp,))] * 4,
        compiler_params=pltpu.CompilerParams(
            collective_id=0, has_side_effects=True, vmem_limit_bytes=56 * 2**20
        ),
    )(
        activations,
        gain,
        down,
        fade,
        decay_up_factor,
        decay_offset_bias.reshape(1, -1),
        head_sink_logit,
        linear_head_gain.reshape(1, -1),
        *matrices,
        starting_state,
    )


def mixer(*arrays):
    sp, tp = lax.axis_size("sp"), lax.axis_size("tp")
    rows = arrays[0].shape[0]
    one_each = KVH == GATED_MIXERS == sp * tp and QH % KVH == 0
    if tp == 2 and sp % tp == 0 and one_each and rows == WINDOW and rows % SPAN == 0:
        return stationary(*arrays)
    return local(*arrays)


def solution(mesh):
    placed = (
        P(("fs", "sp"), "tp"),
        P(),
        P("sp", "tp"),
        P("sp", "tp"),
        P("sp", "tp"),
        P("sp", "tp"),
        P("sp", "tp"),
        P("sp", "tp"),
        P(),
        P(None, "tp"),
        P("tp"),
        P(("fs", "sp"), "tp"),
        P("tp", None, None),
        P("tp"),
        P(),
        P("tp", "sp"),
        P("tp", "sp"),
    )
    return jax.shard_map(
        mixer, mesh=mesh, in_specs=placed, out_specs=P(("fs", "sp", "tp"), None), check_vma=False
    )
```
